32 devices in a mesh: dp: 4 (over y, x), kv: 4 (over z), tp: 2 (over core).
Axes of the slice: x: 2, y: 2, z: 4, core: 2. Of those that a mesh axis runs over, the one named last changes fastest.
Arguments:
- tokens: bfloat16 [32, 2048], P('dp', ('kv', 'tp')), as said below
- first_gain: float32 [2048], replicated, may hold values from 0.1 to 1.9
- first_gate: bfloat16 [2048, 5632], P(None, ('kv', 'tp')), may hold values from -0.125 to 0.125
- first_up: bfloat16 [2048, 5632], P(None, ('kv', 'tp')), may hold values from -0.125 to 0.125
- first_down: bfloat16 [5632, 2048], P(('kv', 'tp')), may hold values from -0.109375 to 0.109375
- mix_gain: float32 [2048], P(('kv', 'tp')), may hold values from 0.1 to 1.9
- w_input: bfloat16 [2048, 2048], P(('kv', 'tp')), may hold values from -0.125 to 0.125
- w_outgate: bfloat16 [2048, 2048], P(('kv', 'tp')), may hold values from -0.125 to 0.125
- w_write: bfloat16 [2048, 512], P(('kv', 'tp')), may hold values from -0.125 to 0.125
- w_read: bfloat16 [2048, 512], P(('kv', 'tp')), may hold values from -0.125 to 0.125
- w_step: bfloat16 [2048, 32], P(('kv', 'tp')), may hold values from -0.125 to 0.125
- conv_taps: bfloat16 [4, 3072], replicated, may hold values from -3 to 3
- conv_history: bfloat16 [32, 3, 3072], P(('dp', 'kv', 'tp')), may hold values from -6 to 6
- step_bias: float32 [32], replicated, may hold values from -6 to -1
- rate_log: float32 [32], replicated, may hold values from 0 to 2.77
- mixer_state: float32 [32, 32, 64, 128], P(('dp', 'kv', 'tp')), may hold values from -4 to 4
- group_gain: float32 [2048], replicated, may hold values from 0.1 to 1.9
- w_output: bfloat16 [2048, 2048], P(None, ('kv', 'tp')), may hold values from -0.125 to 0.125
- second_gain: float32 [2048], replicated, may hold values from 0.1 to 1.9
- second_gate: bfloat16 [2048, 5632], P(None, ('kv', 'tp')), may hold values from -0.125 to 0.125
- second_up: bfloat16 [2048, 5632], P(None, ('kv', 'tp')), may hold values from -0.125 to 0.125
- second_down: bfloat16 [5632, 2048], P(('kv', 'tp')), may hold values from -0.109375 to 0.109375
Outputs:
- layer_out: bfloat16 [32, 2048], P('dp', ('kv', 'tp'))
- state_out: float32 [32, 32, 64, 128], P(('dp', 'kv', 'tp'))
- history_out: bfloat16 [32, 3, 3072], P(('dp', 'kv', 'tp'))
The draws below stay inside these ranges and needn't reach their ends.
Inputs may be any that keep to these rules, and one draw needn't show every extreme that they name: `tokens`: channel scales rise along the width.
All inputs are finite; a program needn't handle non-finite values.
Results may differ from the reference program's by a relative error of at most 0.014.
Values may be sent and summed in bfloat16 or wider, within the bound.
No kernel may reach another device: no remote copies, remote signals or barrier semaphores. Data moves between devices by JAX's collectives and lax.ppermute only.
A program may use at most 64 MiB of HBM per device.

```python
import math
import jax
import jax.numpy as jnp
from jax import lax

D = 2048
FF = 5632
HEADS = 32
HEAD_DIM = 64
D_STATE = 128
GROUPS = 4
TAPS = 4
BATCH = 32
SSD_WIDTH = 2048
CONV_DIM = 3072


def draw_tokens(key, part):
    column = jnp.exp(jnp.linspace(0.0, math.log(6.0), D)).astype(jnp.float32)
    values = jax.random.normal(key, (BATCH, D), jnp.float32) * column / 3.0
    return values.astype(jnp.bfloat16)


def raised(array, stream_key, source, target, shards_of, factor):
    def block_of(position):
        return (jnp.arange(array.shape[position]) // (array.shape[position] // shards_of)).reshape((-1,) + (1,) * (array.ndim - 1 - position))

    first = jax.random.permutation(stream_key, shards_of)[block_of(target)]
    second = (block_of(target) + shards_of // 2) % shards_of
    return jnp.where((block_of(source) == first) | (block_of(source) == second), factor * array, array)


def levels(own_key, shape, shards, low, top_value):
    def one(axis_at, shards_of):
        steps = jax.random.uniform(jax.random.fold_in(jax.random.fold_in(own_key, 6), axis_at), (shards_of,), jnp.float32, low / len(shards), top_value / len(shards))
        return jnp.repeat(jnp.exp(steps), shape[axis_at] // shards_of).reshape((-1,) + (1,) * (len(shape) - axis_at - 1))

    factor_of = one(*shards[0])
    for cut in shards[1:]:
        factor_of = factor_of * one(*cut)
    return factor_of


def bell_draw(key, dims, scale, most, pieces=(), kind=jnp.bfloat16):
    result = jax.random.normal(key, dims, jnp.float32) * scale
    if len(pieces) > 0:
        result = levels(key, dims, pieces, -0.22, 0.18) * result
    return jnp.clip(result, min=-most, max=most).astype(kind)


def noise_with(stream_key, dims, spread, reach, cuts, heavy, dtype=jnp.bfloat16):
    drawn = spread * jax.random.normal(stream_key, dims, jnp.float32)
    if cuts:
        drawn = drawn * levels(stream_key, dims, cuts, -0.22, 0.18)
    return jnp.clip(raised(drawn, jax.random.fold_in(stream_key, 3), *heavy), -reach, reach).astype(dtype)


def setup_inputs(seed: int = 0) -> dict:
    splits = jax.random.split(jax.random.key(seed), 23)
    tokens = draw_tokens(jax.random.fold_in(splits[22], 71), 0)
    first_gain = jnp.clip(1.0 + 0.18 * jax.random.normal(splits[1], (D,), jnp.float32), 0.1, 1.9)
    first_gate = bell_draw(splits[2], (D, FF), D ** -0.5, 0.125, ((1, 8),))
    first_up = bell_draw(splits[3], (D, FF), D ** -0.5, 0.125, ((1, 8),))
    first_down = noise_with(splits[4], (FF, D), FF ** -0.5, 0.109375, ((0, 8),), (0, 1, 8, 2.0))
    mix_gain = jnp.clip(1.0 + 0.18 * jax.random.normal(splits[5], (D,), jnp.float32), 0.1, 1.9)
    w_input = bell_draw(splits[6], (D, SSD_WIDTH), D ** -0.5, 0.125, ((0, 8),))
    w_outgate = bell_draw(splits[7], (D, SSD_WIDTH), D ** -0.5, 0.125, ((0, 8),))
    w_write = bell_draw(splits[8], (D, GROUPS * D_STATE), D ** -0.5, 0.125, ((0, 8),))
    w_read = bell_draw(splits[9], (D, GROUPS * D_STATE), D ** -0.5, 0.125, ((0, 8),))
    w_step = bell_draw(splits[10], (D, HEADS), D ** -0.5, 0.125, ((0, 8),))
    conv_taps = bell_draw(splits[11], (TAPS, CONV_DIM), 0.5, 3.0)
    conv_history = bell_draw(splits[12], (BATCH, TAPS - 1, CONV_DIM), 1.0, 6.0, ((0, 32),))
    step_bias = jnp.clip(jax.random.uniform(splits[13], (HEADS,), jnp.float32, -6.0, -1.0), -6.0, -1.0)
    rate_log = jnp.clip(jax.random.uniform(splits[14], (HEADS,), jnp.float32, 0.0, 2.77), 0.0, 2.77)
    mixer_state = bell_draw(splits[15], (BATCH, HEADS, HEAD_DIM, D_STATE), 0.5, 4.0, ((0, 32),), jnp.float32)
    group_gain = jnp.clip(1.0 + 0.18 * jax.random.normal(splits[16], (SSD_WIDTH,), jnp.float32), 0.1, 1.9)
    w_output = bell_draw(splits[17], (SSD_WIDTH, D), SSD_WIDTH ** -0.5, 0.125, ((1, 8),))
    second_gain = jnp.clip(1.0 + 0.18 * jax.random.normal(splits[18], (D,), jnp.float32), 0.1, 1.9)
    second_gate = bell_draw(splits[19], (D, FF), D ** -0.5, 0.125, ((1, 8),))
    second_up = bell_draw(splits[20], (D, FF), D ** -0.5, 0.125, ((1, 8),))
    second_down = noise_with(splits[21], (FF, D), FF ** -0.5, 0.109375, ((0, 8),), (0, 1, 8, 2.0))
    return dict(tokens=tokens, first_gain=first_gain, first_gate=first_gate, first_up=first_up, first_down=first_down, mix_gain=mix_gain, w_input=w_input, w_outgate=w_outgate, w_write=w_write, w_read=w_read, w_step=w_step, conv_taps=conv_taps, conv_history=conv_history, step_bias=step_bias, rate_log=rate_log, mixer_state=mixer_state, group_gain=group_gain, w_output=w_output, second_gain=second_gain, second_gate=second_gate, second_up=second_up, second_down=second_down)


EPS = 1e-06

def half_block(resid, gain, w_gate, w_up, w_down):
    resid_f = resid.astype(jnp.float32)
    scale = lax.rsqrt(lax.optimization_barrier(jnp.mean(resid_f * resid_f, axis=-1, keepdims=True)) + EPS)
    normed = (resid_f * scale * gain).astype(jnp.bfloat16)
    gate = jnp.dot(normed, w_gate, preferred_element_type=jnp.float32)
    upper = jnp.dot(normed, w_up, preferred_element_type=jnp.float32)
    hidden = (jax.nn.silu(gate) * upper).astype(jnp.bfloat16)
    down = jnp.dot(hidden, w_down, preferred_element_type=jnp.float32)
    return (resid_f + 0.5 * down).astype(jnp.bfloat16)

def reference(tokens, first_gain, first_gate, first_up, first_down, mix_gain, w_input, w_outgate, w_write, w_read, w_step, conv_taps, conv_history, step_bias, rate_log, mixer_state, group_gain, w_output, second_gain, second_gate, second_up, second_down):
    first = half_block(tokens, first_gain, first_gate, first_up, first_down)
    first_f = first.astype(jnp.float32)
    squares = lax.optimization_barrier(jnp.sum(first_f * first_f, axis=1, keepdims=True))
    scale = lax.rsqrt(squares / D + EPS)
    premix = (first_f * mix_gain).astype(jnp.bfloat16)

    def project(weight):
        return (scale * jnp.dot(premix, weight, preferred_element_type=jnp.float32)).astype(jnp.bfloat16)
    inputs = project(w_input)
    outgate = project(w_outgate)
    writes = project(w_write)
    reads = project(w_read)
    steps_raw = project(w_step)
    fresh = jnp.concatenate([inputs, writes, reads], axis=1)
    window = jnp.concatenate([conv_history, fresh[:, None, :]], axis=1)
    history_out = window[:, 1:]
    conv = jax.nn.silu(lax.optimization_barrier(jnp.sum(window.astype(jnp.float32) * conv_taps.astype(jnp.float32)[None], axis=1)))
    count = conv.shape[0]
    per_group = HEADS // GROUPS
    conv_in = conv[:, :SSD_WIDTH].reshape(count, GROUPS, per_group, HEAD_DIM)
    conv_write = conv[:, SSD_WIDTH:SSD_WIDTH + GROUPS * D_STATE].reshape(count, GROUPS, D_STATE)
    conv_read = conv[:, SSD_WIDTH + GROUPS * D_STATE:].reshape(count, GROUPS, D_STATE)
    step = jax.nn.softplus(steps_raw.astype(jnp.float32) + step_bias)
    decay = jnp.exp(-step * jnp.exp(rate_log))
    state = mixer_state.reshape(count, GROUPS, per_group, HEAD_DIM, D_STATE)
    decay_g = decay.reshape(count, GROUPS, per_group)
    step_g = step.reshape(count, GROUPS, per_group)
    written = (step_g[..., None] * conv_in)[..., None] * conv_write[:, :, None, None, :]
    new_state = decay_g[..., None, None] * state + written
    read_out = jnp.einsum('sgjpn,sgn->sgjp', new_state, conv_read, precision=lax.Precision.HIGHEST)
    gated = read_out.reshape(count, SSD_WIDTH) * jax.nn.silu(outgate.astype(jnp.float32))
    blocks = gated.reshape(count, GROUPS, SSD_WIDTH // GROUPS)
    block_scale = lax.rsqrt(lax.optimization_barrier(jnp.mean(blocks * blocks, axis=-1, keepdims=True)) + EPS)
    normed = ((blocks * block_scale).reshape(count, SSD_WIDTH) * group_gain).astype(jnp.bfloat16)
    mixed = jnp.dot(normed, w_output, preferred_element_type=jnp.float32)
    second = (first_f + mixed).astype(jnp.bfloat16)
    layer_out = half_block(second, second_gain, second_gate, second_up, second_down)
    state_out = new_state.reshape(count, HEADS, HEAD_DIM, D_STATE)
    return (layer_out, state_out, history_out)
```

```python
import jax
import jax.numpy as jnp
from jax import lax
from jax.sharding import PartitionSpec as P

EPS = 1e-06
AXES = ("kv", "tp")


def exchange(blocks):
    return lax.all_to_all(blocks, AXES, split_axis=0, concat_axis=0, tiled=True)


def gather(block, ways):
    return exchange(jnp.broadcast_to(block[None], (ways,) + block.shape))


def scatter_sum(partial, ways):
    rows, width = partial.shape
    blocks = partial.reshape(rows, ways, width // ways).transpose(1, 0, 2)
    return jnp.sum(exchange(blocks), axis=0)


def half_block(resid, gain, w_gate, w_up, w_down, ways):
    rows = resid.shape[0]
    whole = gather(resid, ways).transpose(1, 0, 2).reshape(rows, -1)
    whole_f = whole.astype(jnp.float32)
    scale = lax.rsqrt(jnp.mean(whole_f * whole_f, axis=-1, keepdims=True) + EPS)
    normed = (whole_f * scale * gain).astype(jnp.bfloat16)
    gate = jnp.dot(normed, w_gate, preferred_element_type=jnp.float32)
    upper = jnp.dot(normed, w_up, preferred_element_type=jnp.float32)
    hidden = (jax.nn.silu(gate) * upper).astype(jnp.bfloat16)
    down = jnp.dot(hidden, w_down, preferred_element_type=jnp.float32)
    share = scatter_sum(down, ways)
    return (resid.astype(jnp.float32) + 0.5 * share).astype(jnp.bfloat16)


def make_body(ways):
    def body(
        tokens,
        first_gain,
        first_gate,
        first_up,
        first_down,
        mix_gain,
        w_input,
        w_outgate,
        w_write,
        w_read,
        w_step,
        conv_taps,
        conv_history,
        step_bias,
        rate_log,
        mixer_state,
        group_gain,
        w_output,
        second_gain,
        second_gate,
        second_up,
        second_down,
    ):
        width = first_gate.shape[0]
        count = mixer_state.shape[0]
        heads = mixer_state.shape[1]
        head_dim = mixer_state.shape[2]
        state_dim = mixer_state.shape[3]
        ssd_width = heads * head_dim
        groups = w_write.shape[1] // state_dim
        per_group = heads // groups
        rows = tokens.shape[0]
        first = half_block(tokens, first_gain, first_gate, first_up, first_down, ways)
        first_f = first.astype(jnp.float32)
        squares = jnp.sum(first_f * first_f, axis=1, keepdims=True)
        premix = (first_f * mix_gain).astype(jnp.bfloat16)
        parts = [
            jnp.dot(premix, w, preferred_element_type=jnp.float32)
            for w in (w_input, w_write, w_read, w_outgate, w_step)
        ]
        ends = []
        total = 0
        for p in parts:
            total += p.shape[1]
            ends.append(total)
        padded = -(-(total + 1) // 1024) * 1024
        pad = jnp.zeros((rows, padded - total - 1), jnp.float32)
        packed = jnp.concatenate(parts + [squares, pad], axis=1)
        packed = packed.reshape(ways, count, padded)
        summed = jnp.sum(exchange(packed), axis=0)
        own_squares = summed[:, total : total + 1]
        scale = lax.rsqrt(own_squares / width + EPS)
        scaled = (scale * summed[:, :total]).astype(jnp.bfloat16)
        fresh = scaled[:, : ends[2]]
        outgate = scaled[:, ends[2] : ends[3]]
        steps_raw = scaled[:, ends[3] :]
        window = jnp.concatenate([conv_history, fresh[:, None, :]], axis=1)
        history_out = window[:, 1:]
        conv = jax.nn.silu(
            jnp.sum(window.astype(jnp.float32) * conv_taps.astype(jnp.float32)[None], axis=1)
        )
        conv_in = conv[:, :ssd_width].reshape(count, groups, per_group, head_dim)
        conv_write = conv[:, ssd_width : ssd_width + groups * state_dim].reshape(
            count, groups, state_dim
        )
        conv_read = conv[:, ssd_width + groups * state_dim :].reshape(count, groups, state_dim)
        step = jax.nn.softplus(steps_raw.astype(jnp.float32) + step_bias)
        decay = jnp.exp(-step * jnp.exp(rate_log))
        state = mixer_state.reshape(count, groups, per_group, head_dim, state_dim)
        decay_g = decay.reshape(count, groups, per_group)
        step_g = step.reshape(count, groups, per_group)
        written = (step_g[..., None] * conv_in)[..., None] * conv_write[:, :, None, None, :]
        new_state = decay_g[..., None, None] * state + written
        read_out = jnp.sum(new_state * conv_read[:, :, None, None, :], axis=-1)
        gated = read_out.reshape(count, ssd_width) * jax.nn.silu(outgate.astype(jnp.float32))
        blocks = gated.reshape(count, groups, ssd_width // groups)
        block_scale = lax.rsqrt(jnp.mean(blocks * blocks, axis=-1, keepdims=True) + EPS)
        normed = ((blocks * block_scale).reshape(count, ssd_width) * group_gain).astype(jnp.bfloat16)
        mixed = jnp.dot(
            gather(normed, ways).reshape(rows, ssd_width),
            w_output,
            preferred_element_type=jnp.float32,
        )
        second = (first_f + mixed).astype(jnp.bfloat16)
        layer_out = half_block(second, second_gain, second_gate, second_up, second_down, ways)
        state_out = new_state.reshape(count, heads, head_dim, state_dim)
        return (layer_out, state_out, history_out)

    return body


def solution(mesh):
    whole = P(AXES)
    rows = P(AXES, None)
    columns = P(None, AXES)
    own = ("dp",) + AXES
    return jax.shard_map(
        make_body(mesh.shape["kv"] * mesh.shape["tp"]),
        mesh=mesh,
        in_specs=(
            P("dp", AXES),
            P(),
            columns,
            columns,
            rows,
            whole,
            rows,
            rows,
            rows,
            rows,
            rows,
            P(),
            P(own, None, None),
            P(),
            P(),
            P(own, None, None, None),
            P(),
            columns,
            P(),
            columns,
            columns,
            rows,
        ),
        out_specs=(P("dp", AXES), P(own, None, None, None), P(own, None, None)),
        check_vma=False,
    )
```

```python
import functools

import jax
import jax.numpy as jnp
from jax import lax
from jax.experimental import pallas as pl
from jax.experimental.pallas import tpu as pltpu
from jax.sharding import PartitionSpec as P

EPS = 1e-06
AXES = ("kv", "tp")
LANES = 128
MIB = 1 << 20
VMEM_SPEC = pl.BlockSpec(memory_space=pltpu.VMEM)
ANY_SPEC = pl.BlockSpec(memory_space=pl.ANY)
ROW_ROW = (((1,), (1,)), ((), ()))


def exchange(blocks):
    return lax.all_to_all(blocks, AXES, split_axis=0, concat_axis=0, tiled=True)


def params(megabytes):
    return pltpu.CompilerParams(vmem_limit_bytes=megabytes * MIB)


def cost(nbytes):
    return pl.CostEstimate(flops=nbytes, bytes_accessed=nbytes, transcendentals=0)


def silu(x):
    return x / (1.0 + jnp.exp(-x))


def load_kernel(cuts, *refs):
    n = len(cuts)
    sources, targets, sems = refs[:n], refs[n : 2 * n], refs[2 * n]
    copies = []
    for source, target, cut in zip(sources, targets, cuts):
        step = source.shape[0] // cut
        for i in range(cut):
            part = pl.ds(i * step, step)
            copies.append(
                pltpu.make_async_copy(source.at[part], target.at[part], sems.at[len(copies)])
            )
    for copy in copies:
        copy.start()
    for copy in copies:
        copy.wait()


def load(*arrays):
    cuts = tuple(4 if a.size * a.dtype.itemsize >= MIB and a.shape[0] % 64 == 0 else 1 for a in arrays)
    return pl.pallas_call(
        functools.partial(load_kernel, cuts),
        out_shape=[pltpu.VMEM(a.shape, a.dtype) for a in arrays],
        in_specs=[ANY_SPEC] * len(arrays),
        out_specs=[VMEM_SPEC] * len(arrays),
        scratch_shapes=[pltpu.SemaphoreType.DMA((sum(cuts),))],
        compiler_params=params(4),
        cost_estimate=cost(sum(a.size * a.dtype.itemsize for a in arrays)),
    )(*arrays)


def ff_kernel(x_ref, gain_ref, gate_ref, up_ref, down_hbm, out_ref, down_ref, sem):
    copy = pltpu.make_async_copy(down_hbm, down_ref, sem)
    copy.start()
    ways, rows, chan = x_ref.shape
    pieces = [x_ref[k].astype(jnp.float32) for k in range(ways)]
    total = jnp.zeros((rows, 1), jnp.float32)
    for piece in pieces:
        total += jnp.sum(piece * piece, axis=1, keepdims=True)
    scale = lax.rsqrt(total / (ways * chan) + EPS)
    normed = jnp.concatenate(
        [
            (piece * scale * gain_ref[:, k * chan : (k + 1) * chan]).astype(jnp.bfloat16)
            for k, piece in enumerate(pieces)
        ],
        axis=1,
    )
    gate = lax.dot_general(normed, gate_ref[...], ROW_ROW, preferred_element_type=jnp.float32)
    upper = lax.dot_general(normed, up_ref[...], ROW_ROW, preferred_element_type=jnp.float32)
    hidden = (silu(gate) * upper).astype(jnp.bfloat16)
    copy.wait()
    down = jnp.dot(hidden, down_ref[...], preferred_element_type=jnp.float32)
    for k in range(ways):
        out_ref[k] = down[:, k * chan : (k + 1) * chan]


def ff_loaded_kernel(x_ref, gain_ref, gate_ref, up_ref, down_ref, out_ref):
    ways, rows, chan = x_ref.shape
    pieces = [x_ref[k].astype(jnp.float32) for k in range(ways)]
    total = jnp.zeros((rows, 1), jnp.float32)
    for piece in pieces:
        total += jnp.sum(piece * piece, axis=1, keepdims=True)
    scale = lax.rsqrt(total / (ways * chan) + EPS)
    normed = jnp.concatenate(
        [
            (piece * scale * gain_ref[:, k * chan : (k + 1) * chan]).astype(jnp.bfloat16)
            for k, piece in enumerate(pieces)
        ],
        axis=1,
    )
    gate = lax.dot_general(normed, gate_ref[...], ROW_ROW, preferred_element_type=jnp.float32)
    upper = lax.dot_general(normed, up_ref[...], ROW_ROW, preferred_element_type=jnp.float32)
    hidden = (silu(gate) * upper).astype(jnp.bfloat16)
    down = jnp.dot(hidden, down_ref[...], preferred_element_type=jnp.float32)
    for k in range(ways):
        out_ref[k] = down[:, k * chan : (k + 1) * chan]


def ff(whole, gain, gate, up, down, loaded):
    size = 3 * gate.size * 2
    scratch = [] if loaded else [pltpu.VMEM(down.shape, down.dtype), pltpu.SemaphoreType.DMA]
    return pl.pallas_call(
        ff_loaded_kernel if loaded else ff_kernel,
        out_shape=jax.ShapeDtypeStruct(whole.shape, jnp.float32),
        in_specs=[VMEM_SPEC] * 4 + [VMEM_SPEC if loaded else ANY_SPEC],
        out_specs=VMEM_SPEC,
        scratch_shapes=scratch,
        compiler_params=params(8),
        cost_estimate=cost(size),
    )(whole, gain, gate, up, down)


def project_kernel(got_ref, tok_ref, gain_ref, win_ref, wwrite_ref, wread_ref, wgate_ref, wstep_ref,
                   first_ref, out_ref, stage):
    ways, rows, _ = got_ref.shape
    slots = out_ref.shape[1]
    share = got_ref[0]
    for k in range(1, ways):
        share += got_ref[k]
    first = (tok_ref[...].astype(jnp.float32) + 0.5 * share).astype(jnp.bfloat16)
    first_ref[...] = first
    first_f = first.astype(jnp.float32)
    squares = jnp.sum(first_f * first_f, axis=1, keepdims=True)
    premix = (first_f * gain_ref[...]).astype(jnp.bfloat16)
    row = 0
    for w_ref in (win_ref, wwrite_ref, wread_ref, wgate_ref):
        part = jnp.dot(premix, w_ref[...], preferred_element_type=jnp.float32)
        for j in range(part.shape[1] // LANES):
            stage[pl.ds(row, rows, stride=slots), :] = part[:, j * LANES : (j + 1) * LANES]
            row += 1
    steps = lax.dot_general(premix, wstep_ref[...], ROW_ROW, preferred_element_type=jnp.float32)
    stage[pl.ds(row, rows, stride=slots), :] = jnp.zeros((rows, LANES), jnp.float32)
    stage[pl.ds(row, rows, stride=slots), : steps.shape[1]] = steps
    row += 1
    rest = jnp.broadcast_to(squares, (rows, LANES))
    for _ in range(3):
        term = rest.astype(jnp.bfloat16).astype(jnp.float32)
        stage[pl.ds(row, rows, stride=slots), :] = term
        rest = rest - term
        row += 1
    for j in range(row, slots):
        stage[pl.ds(j, rows, stride=slots), :] = jnp.zeros((rows, LANES), jnp.float32)
    for s in range(rows):
        out_ref[s] = stage[pl.ds(s * slots, slots), :].astype(jnp.bfloat16)


def project(got, tokens, gain, w_in, w_write, w_read, w_gate, w_step, slots):
    _, rows, chan = got.shape
    size = 2 * (w_in.size + w_write.size + w_read.size + w_gate.size)
    return pl.pallas_call(
        project_kernel,
        out_shape=[
            jax.ShapeDtypeStruct((rows, chan), jnp.bfloat16),
            jax.ShapeDtypeStruct((rows, slots, LANES), jnp.bfloat16),
        ],
        in_specs=[VMEM_SPEC] * 8,
        out_specs=[VMEM_SPEC] * 2,
        scratch_shapes=[pltpu.VMEM((rows * slots, LANES), jnp.float32)],
        compiler_params=params(8),
        cost_estimate=cost(size),
    )(got, tokens, gain, w_in, w_write, w_read, w_gate, w_step)


def spread_kernel(wide_ref, out_ref):
    taps, width = wide_ref.shape
    slots = width // LANES
    for j in range(slots):
        out_ref[pl.ds(j, taps, stride=slots), :] = wide_ref[:, j * LANES : (j + 1) * LANES].astype(
            jnp.float32
        )


def spread(wide):
    taps, width = wide.shape
    return pl.pallas_call(
        spread_kernel,
        out_shape=pltpu.VMEM((taps * width // LANES, LANES), jnp.float32),
        in_specs=[VMEM_SPEC],
        out_specs=VMEM_SPEC,
        compiler_params=params(2),
    )(wide)


def mixer_kernel(width, groups, got_ref, taps_ref, hist_ref, bias_ref, rate_ref, state_ref, ggain_ref,
                 state_out_ref, fresh_ref, normed_ref, read_rows):
    ways = got_ref.shape[0]
    heads, head_dim, state_dim = state_ref.shape
    in_rows = heads * head_dim // LANES
    map_rows = groups * state_dim // LANES
    conv_rows = in_rows + 2 * map_rows
    taps = taps_ref.shape[0] // conv_rows
    total = got_ref[0].astype(jnp.float32)
    for k in range(1, ways):
        total += got_ref[k].astype(jnp.float32)
    step_row = conv_rows + in_rows
    squares = (
        total[step_row + 1 : step_row + 2]
        + total[step_row + 2 : step_row + 3]
        + total[step_row + 3 : step_row + 4]
    )
    scale = lax.rsqrt(squares / width + EPS)
    rounded = (total * scale).astype(jnp.bfloat16).astype(jnp.float32)
    fresh = rounded[:conv_rows]
    fresh_ref[...] = fresh.astype(jnp.bfloat16)
    acc = hist_ref[pl.ds(0, conv_rows), :] * taps_ref[pl.ds(0, conv_rows), :]
    for k in range(1, taps - 1):
        part = pl.ds(k * conv_rows, conv_rows)
        acc += hist_ref[part, :] * taps_ref[part, :]
    acc += fresh * taps_ref[pl.ds((taps - 1) * conv_rows, conv_rows), :]
    conv = silu(acc)
    maps = conv[in_rows:]
    raw = rounded[step_row : step_row + 1] + bias_ref[...]
    step = jnp.maximum(raw, 0.0) + jnp.log1p(jnp.exp(-jnp.abs(raw)))
    decay = jnp.exp(-step * jnp.exp(rate_ref[...]))
    pad = jnp.zeros((LANES - in_rows, LANES), jnp.float32)
    columns = jnp.concatenate([conv[:in_rows], pad], axis=0).T
    per_row = LANES // head_dim
    per_group = heads // groups
    for g in range(groups):
        write = maps[g : g + 1]
        for h in range(g * per_group, (g + 1) * per_group):
            r, c = h // per_row, h % per_row
            column = columns[c * head_dim : (c + 1) * head_dim, r : r + 1] * step[:, h : h + 1]
            state_out_ref[h] = decay[:, h : h + 1] * state_ref[h] + column * write
        block = state_out_ref[g * per_group : (g + 1) * per_group].reshape(
            per_group * head_dim, state_dim
        )
        read = lax.dot_general(
            maps,
            block,
            ROW_ROW,
            precision=lax.Precision.HIGHEST,
            preferred_element_type=jnp.float32,
        )
        span = per_group * head_dim // LANES
        for j in range(span):
            read_rows[g * span + j : g * span + j + 1, :] = read[
                map_rows + g : map_rows + g + 1, j * LANES : (j + 1) * LANES
            ]
    gated = read_rows[...] * silu(rounded[conv_rows : conv_rows + in_rows])
    sums = jnp.sum(gated * gated, axis=1, keepdims=True)
    owner = lax.broadcasted_iota(jnp.int32, (in_rows, 1), 0) // (in_rows // groups)
    block_scale = jnp.zeros((in_rows, 1), jnp.float32)
    for g in range(groups):
        mine = owner == g
        mean = jnp.sum(jnp.where(mine, sums, 0.0), axis=0, keepdims=True) / (
            in_rows // groups * LANES
        )
        block_scale = jnp.where(mine, lax.rsqrt(mean + EPS), block_scale)
    normed = (gated * block_scale * ggain_ref[...]).astype(jnp.bfloat16)
    for k in range(ways):
        normed_ref[k] = normed


def mixer(width, groups, got, taps, hist, bias, rate, state, ggain):
    ways = got.shape[0]
    heads, head_dim, state_dim = state.shape
    in_rows = heads * head_dim // LANES
    conv_rows = in_rows + 2 * groups * state_dim // LANES
    return pl.pallas_call(
        functools.partial(mixer_kernel, width, groups),
        out_shape=[
            pltpu.VMEM(state.shape, jnp.float32),
            jax.ShapeDtypeStruct((conv_rows, LANES), jnp.bfloat16),
            jax.ShapeDtypeStruct((ways, in_rows, LANES), jnp.bfloat16),
        ],
        in_specs=[VMEM_SPEC] * 7,
        out_specs=[VMEM_SPEC] * 3,
        scratch_shapes=[pltpu.VMEM((in_rows, LANES), jnp.float32)],
        compiler_params=params(8),
        cost_estimate=cost(8 * state.size),
    )(got, taps, hist, bias, rate, state, ggain)


def store_kernel(source, target, sems):
    cut = sems.shape[0]
    step = source.shape[0] // cut
    copies = [
        pltpu.make_async_copy(
            source.at[pl.ds(i * step, step)], target.at[pl.ds(i * step, step)], sems.at[i]
        )
        for i in range(cut)
    ]
    for copy in copies:
        copy.start()
    for copy in copies:
        copy.wait()


def store(array):
    return pl.pallas_call(
        store_kernel,
        out_shape=pltpu.HBM(array.shape, array.dtype),
        in_specs=[VMEM_SPEC],
        out_specs=pl.BlockSpec(memory_space=pltpu.HBM),
        scratch_shapes=[pltpu.SemaphoreType.DMA((4,))],
        compiler_params=params(2),
        cost_estimate=cost(array.size * array.dtype.itemsize),
    )(array)


def output_kernel(got_ref, w_ref, first_ref, out_ref, stage):
    ways, slots, _ = got_ref.shape
    for k in range(ways):
        stage[pl.ds(k * slots, slots), :] = got_ref[k].astype(jnp.float32)
    rows = jnp.concatenate(
        [stage[pl.ds(j, ways, stride=slots), :].astype(jnp.bfloat16) for j in range(slots)], axis=1
    )
    mixed = jnp.dot(rows, w_ref[...], preferred_element_type=jnp.float32)
    second = (first_ref[...].astype(jnp.float32) + mixed).astype(jnp.bfloat16)
    for k in range(ways):
        out_ref[k] = second


def output(got, w, first):
    ways, slots, _ = got.shape
    return pl.pallas_call(
        output_kernel,
        out_shape=jax.ShapeDtypeStruct((ways,) + first.shape, jnp.bfloat16),
        in_specs=[VMEM_SPEC] * 3,
        out_specs=VMEM_SPEC,
        scratch_shapes=[pltpu.VMEM((ways * slots, LANES), jnp.float32)],
        compiler_params=params(4),
        cost_estimate=cost(2 * w.size),
    )(got, w, first)


def final_kernel(got_ref, second_ref, out_ref):
    share = got_ref[0]
    for k in range(1, got_ref.shape[0]):
        share += got_ref[k]
    out_ref[...] = (second_ref[0].astype(jnp.float32) + 0.5 * share).astype(jnp.bfloat16)


def final(got, second_all):
    return pl.pallas_call(
        final_kernel,
        out_shape=jax.ShapeDtypeStruct(second_all.shape[1:], jnp.bfloat16),
        in_specs=[VMEM_SPEC] * 2,
        out_specs=VMEM_SPEC,
        compiler_params=params(2),
    )(got, second_all)


def fast_body(
    ways,
    tokens,
    first_gain,
    first_gate,
    first_up,
    first_down,
    mix_gain,
    w_input,
    w_outgate,
    w_write,
    w_read,
    w_step,
    conv_taps,
    conv_history,
    step_bias,
    rate_log,
    mixer_state,
    group_gain,
    w_output,
    second_gain,
    second_gate,
    second_up,
    second_down,
):
    width = first_gate.shape[0]
    _, heads, head_dim, state_dim = mixer_state.shape
    groups = w_write.shape[1] // state_dim
    conv_width = conv_taps.shape[1]
    used = (conv_width + heads * head_dim) // LANES + 4
    slots = -(-used // 16) * 16
    lane_pad = (0, LANES - heads)

    gate1, up1, gain1 = load(first_gate.T, first_up.T, first_gain.reshape(1, width))
    whole = exchange(jnp.broadcast_to(tokens[None], (ways,) + tokens.shape))
    down1 = ff(whole, gain1, gate1, up1, first_down, False)
    tok, gain_m, w_in, w_wr, w_rd, w_og, w_st, gate2 = load(
        tokens, mix_gain.reshape(1, -1), w_input, w_write, w_read, w_outgate, w_step.T, second_gate.T
    )
    got1 = exchange(down1)
    first, packed = project(got1, tok, gain_m, w_in, w_wr, w_rd, w_og, w_st, slots)
    state, w_o, up2, taps_w, hist_w, bias, rate, ggain = load(
        mixer_state[0],
        w_output,
        second_up.T,
        conv_taps,
        conv_history[0],
        jnp.pad(step_bias, lane_pad).reshape(1, LANES),
        jnp.pad(rate_log, lane_pad).reshape(1, LANES),
        group_gain.reshape(-1, LANES),
    )
    taps = spread(taps_w)
    hist = spread(hist_w)
    got2 = exchange(packed)
    new_state, fresh, normed = mixer(width, groups, got2, taps, hist, bias, rate, state, ggain)
    down2, gain2 = load(second_down, second_gain.reshape(1, width))
    got3 = exchange(normed)
    second_all = output(got3, w_o, first)
    state_out = store(new_state)
    whole2 = exchange(second_all)
    parts2 = ff(whole2, gain2, gate2, up2, down2, True)
    got4 = exchange(parts2)
    history_out = jnp.concatenate([conv_history[:, 1:], fresh.reshape(1, 1, conv_width)], axis=1)
    layer_out = final(got4, second_all)
    return layer_out, state_out[None], history_out


def friendly(ways, args):
    tokens, gate, taps, state, w_write = args[0], args[2], args[11], args[15], args[8]
    count, heads, head_dim, state_dim = state.shape
    return (
        count == 1
        and tokens.shape[0] == ways == 8
        and tokens.shape[1] % LANES == 0
        and gate.shape[1] % 64 == 0
        and taps.shape[1] % (8 * LANES) == 0
        and state_dim == LANES
        and LANES % head_dim == 0
        and heads < LANES
        and 2 * (w_write.shape[1] // state_dim) == 8
        and heads * head_dim % (16 * LANES) == 0
    )


def gather(block, ways):
    return exchange(jnp.broadcast_to(block[None], (ways,) + block.shape))


def scatter_sum(partial, ways):
    rows, width = partial.shape
    blocks = partial.reshape(rows, ways, width // ways).transpose(1, 0, 2)
    return jnp.sum(exchange(blocks), axis=0)


def half_block(resid, gain, w_gate, w_up, w_down, ways):
    rows = resid.shape[0]
    whole = gather(resid, ways).transpose(1, 0, 2).reshape(rows, -1)
    whole_f = whole.astype(jnp.float32)
    scale = lax.rsqrt(jnp.mean(whole_f * whole_f, axis=-1, keepdims=True) + EPS)
    normed = (whole_f * scale * gain).astype(jnp.bfloat16)
    gate = jnp.dot(normed, w_gate, preferred_element_type=jnp.float32)
    upper = jnp.dot(normed, w_up, preferred_element_type=jnp.float32)
    hidden = (jax.nn.silu(gate) * upper).astype(jnp.bfloat16)
    down = jnp.dot(hidden, w_down, preferred_element_type=jnp.float32)
    share = scatter_sum(down, ways)
    return (resid.astype(jnp.float32) + 0.5 * share).astype(jnp.bfloat16)


def make_plain(ways):
    def body(
        tokens,
        first_gain,
        first_gate,
        first_up,
        first_down,
        mix_gain,
        w_input,
        w_outgate,
        w_write,
        w_read,
        w_step,
        conv_taps,
        conv_history,
        step_bias,
        rate_log,
        mixer_state,
        group_gain,
        w_output,
        second_gain,
        second_gate,
        second_up,
        second_down,
    ):
        width = first_gate.shape[0]
        count = mixer_state.shape[0]
        heads = mixer_state.shape[1]
        head_dim = mixer_state.shape[2]
        state_dim = mixer_state.shape[3]
        ssd_width = heads * head_dim
        groups = w_write.shape[1] // state_dim
        per_group = heads // groups
        rows = tokens.shape[0]
        first = half_block(tokens, first_gain, first_gate, first_up, first_down, ways)
        first_f = first.astype(jnp.float32)
        squares = jnp.sum(first_f * first_f, axis=1, keepdims=True)
        premix = (first_f * mix_gain).astype(jnp.bfloat16)
        parts = [
            jnp.dot(premix, w, preferred_element_type=jnp.float32)
            for w in (w_input, w_write, w_read, w_outgate, w_step)
        ]
        ends = []
        total = 0
        for p in parts:
            total += p.shape[1]
            ends.append(total)
        padded = -(-(total + 1) // 1024) * 1024
        pad = jnp.zeros((rows, padded - total - 1), jnp.float32)
        packed = jnp.concatenate(parts + [squares, pad], axis=1)
        packed = packed.reshape(ways, count, padded)
        summed = jnp.sum(exchange(packed), axis=0)
        own_squares = summed[:, total : total + 1]
        scale = lax.rsqrt(own_squares / width + EPS)
        scaled = (scale * summed[:, :total]).astype(jnp.bfloat16)
        fresh = scaled[:, : ends[2]]
        outgate = scaled[:, ends[2] : ends[3]]
        steps_raw = scaled[:, ends[3] :]
        window = jnp.concatenate([conv_history, fresh[:, None, :]], axis=1)
        history_out = window[:, 1:]
        conv = jax.nn.silu(
            jnp.sum(window.astype(jnp.float32) * conv_taps.astype(jnp.float32)[None], axis=1)
        )
        conv_in = conv[:, :ssd_width].reshape(count, groups, per_group, head_dim)
        conv_write = conv[:, ssd_width : ssd_width + groups * state_dim].reshape(
            count, groups, state_dim
        )
        conv_read = conv[:, ssd_width + groups * state_dim :].reshape(count, groups, state_dim)
        step = jax.nn.softplus(steps_raw.astype(jnp.float32) + step_bias)
        decay = jnp.exp(-step * jnp.exp(rate_log))
        state = mixer_state.reshape(count, groups, per_group, head_dim, state_dim)
        decay_g = decay.reshape(count, groups, per_group)
        step_g = step.reshape(count, groups, per_group)
        written = (step_g[..., None] * conv_in)[..., None] * conv_write[:, :, None, None, :]
        new_state = decay_g[..., None, None] * state + written
        read_out = jnp.sum(new_state * conv_read[:, :, None, None, :], axis=-1)
        gated = read_out.reshape(count, ssd_width) * jax.nn.silu(outgate.astype(jnp.float32))
        blocks = gated.reshape(count, groups, ssd_width // groups)
        block_scale = lax.rsqrt(jnp.mean(blocks * blocks, axis=-1, keepdims=True) + EPS)
        normed = ((blocks * block_scale).reshape(count, ssd_width) * group_gain).astype(jnp.bfloat16)
        mixed = jnp.dot(
            gather(normed, ways).reshape(rows, ssd_width),
            w_output,
            preferred_element_type=jnp.float32,
        )
        second = (first_f + mixed).astype(jnp.bfloat16)
        layer_out = half_block(second, second_gain, second_gate, second_up, second_down, ways)
        state_out = new_state.reshape(count, heads, head_dim, state_dim)
        return (layer_out, state_out, history_out)

    return body


def solution(mesh):
    whole = P(AXES)
    rows = P(AXES, None)
    columns = P(None, AXES)
    own = ("dp",) + AXES
    ways = mesh.shape["kv"] * mesh.shape["tp"]
    plain = make_plain(ways)

    def body(*args):
        if friendly(ways, args):
            return fast_body(ways, *args)
        return plain(*args)

    return jax.shard_map(
        body,
        mesh=mesh,
        in_specs=(
            P("dp", AXES),
            P(),
            columns,
            columns,
            rows,
            whole,
            rows,
            rows,
            rows,
            rows,
            rows,
            P(),
            P(own, None, None),
            P(),
            P(),
            P(own, None, None, None),
            P(),
            columns,
            P(),
            columns,
            columns,
            rows,
        ),
        out_specs=(P("dp", AXES), P(own, None, None, None), P(own, None, None)),
        check_vma=False,
    )
```

```python
import functools

import jax
import jax.numpy as jnp
from jax import lax
from jax.experimental import pallas as pl
from jax.experimental.pallas import tpu as pltpu
from jax.sharding import PartitionSpec as P

EPS = 1e-06
AXES = ("kv", "tp")
LANES = 128
MIB = 1 << 20
VMEM_SPEC = pl.BlockSpec(memory_space=pltpu.VMEM)
ROW_ROW = (((1,), (1,)), ((), ()))


def exchange(blocks):
    return lax.all_to_all(blocks, AXES, split_axis=0, concat_axis=0, tiled=True)


def params(megabytes):
    return pltpu.CompilerParams(vmem_limit_bytes=megabytes * MIB)


COST = pl.CostEstimate(flops=10**10, bytes_accessed=1000, transcendentals=0)


def silu(x):
    return x / (1.0 + jnp.exp(-x))


def repeat_kernel(block_ref, out_ref):
    for k in range(out_ref.shape[0]):
        out_ref[k] = block_ref[...]


def repeat(block, ways):
    return pl.pallas_call(
        repeat_kernel,
        out_shape=jax.ShapeDtypeStruct((ways,) + block.shape, block.dtype),
        in_specs=[VMEM_SPEC],
        out_specs=VMEM_SPEC,
        compiler_params=params(2),
        cost_estimate=COST,
    )(block)


def ff_kernel(x_ref, gain_ref, gate_ref, up_ref, down_ref, out_ref):
    ways, rows, chan = x_ref.shape
    pieces = [x_ref[k].astype(jnp.float32) for k in range(ways)]
    total = jnp.zeros((rows, 1), jnp.float32)
    for piece in pieces:
        total += jnp.sum(piece * piece, axis=1, keepdims=True)
    scale = lax.rsqrt(total / (ways * chan) + EPS)
    normed = jnp.concatenate(
        [
            (piece * scale * gain_ref[:, k * chan : (k + 1) * chan]).astype(jnp.bfloat16)
            for k, piece in enumerate(pieces)
        ],
        axis=1,
    )
    gate = lax.dot_general(normed, gate_ref[...], ROW_ROW, preferred_element_type=jnp.float32)
    upper = lax.dot_general(normed, up_ref[...], ROW_ROW, preferred_element_type=jnp.float32)
    hidden = (silu(gate) * upper).astype(jnp.bfloat16)
    down = jnp.dot(hidden, down_ref[...], preferred_element_type=jnp.float32)
    for k in range(ways):
        out_ref[k] = down[:, k * chan : (k + 1) * chan]


def ff(whole, gain, gate, up, down):
    return pl.pallas_call(
        ff_kernel,
        out_shape=jax.ShapeDtypeStruct(whole.shape, jnp.float32),
        in_specs=[VMEM_SPEC] * 5,
        out_specs=VMEM_SPEC,
        compiler_params=params(8),
        cost_estimate=COST,
    )(whole, gain, gate, up, down)


def project_kernel(got_ref, tok_ref, gain_ref, win_ref, wwrite_ref, wread_ref, wgate_ref, wstep_ref,
                   first_ref, out_ref, stage):
    ways, rows, chan = got_ref.shape
    slots = out_ref.shape[1]
    share = got_ref[0]
    for k in range(1, ways):
        share += got_ref[k]
    first = (tok_ref[...].astype(jnp.float32) + 0.5 * share).astype(jnp.bfloat16)
    first_ref[...] = first
    first_f = first.astype(jnp.float32)
    squares = jnp.sum(first_f * first_f, axis=1, keepdims=True)
    premix = (first_f * gain_ref[...]).astype(jnp.bfloat16)
    row = 0
    for w_ref in (win_ref, wwrite_ref, wread_ref, wgate_ref):
        part = jnp.dot(premix, w_ref[...], preferred_element_type=jnp.float32)
        for j in range(part.shape[1] // LANES):
            stage[pl.ds(row, rows, stride=slots), :] = part[:, j * LANES : (j + 1) * LANES]
            row += 1
    steps = lax.dot_general(premix, wstep_ref[...], ROW_ROW, preferred_element_type=jnp.float32)
    stage[pl.ds(row, rows, stride=slots), :] = jnp.zeros((rows, LANES), jnp.float32)
    stage[pl.ds(row, rows, stride=slots), : steps.shape[1]] = steps
    row += 1
    rest = jnp.broadcast_to(squares, (rows, LANES))
    for _ in range(3):
        term = rest.astype(jnp.bfloat16).astype(jnp.float32)
        stage[pl.ds(row, rows, stride=slots), :] = term
        rest = rest - term
        row += 1
    for j in range(row, slots):
        stage[pl.ds(j, rows, stride=slots), :] = jnp.zeros((rows, LANES), jnp.float32)
    for s in range(rows):
        out_ref[s] = stage[pl.ds(s * slots, slots), :].astype(jnp.bfloat16)


def project(got, tokens, gain, w_in, w_write, w_read, w_gate, w_step, slots):
    ways, rows, chan = got.shape
    return pl.pallas_call(
        project_kernel,
        out_shape=[
            jax.ShapeDtypeStruct((rows, chan), jnp.bfloat16),
            jax.ShapeDtypeStruct((rows, slots, LANES), jnp.bfloat16),
        ],
        in_specs=[VMEM_SPEC] * 8,
        out_specs=[VMEM_SPEC] * 2,
        scratch_shapes=[pltpu.VMEM((rows * slots, LANES), jnp.float32)],
        compiler_params=params(8),
        cost_estimate=COST,
    )(got, tokens, gain, w_in, w_write, w_read, w_gate, w_step)


def mixer_kernel(width, groups, got_ref, taps_ref, hist_ref, bias_ref, rate_ref, state_ref, ggain_ref,
                 state_out_ref, hist_out_ref, normed_ref, read_rows, taps_rows, hist_rows, hist_wide):
    ways = got_ref.shape[0]
    heads, head_dim, state_dim = state_ref.shape
    in_rows = heads * head_dim // LANES
    map_rows = groups * state_dim // LANES
    conv_rows = in_rows + 2 * map_rows
    taps = taps_ref.shape[0]
    for j in range(conv_rows):
        part = pl.ds(j * LANES, LANES)
        taps_rows[pl.ds(j, taps, stride=conv_rows), :] = taps_ref[:, part].astype(jnp.float32)
        hist_rows[pl.ds(j, taps - 1, stride=conv_rows), :] = hist_ref[:, part].astype(jnp.float32)
    total = got_ref[0].astype(jnp.float32)
    for k in range(1, ways):
        total += got_ref[k].astype(jnp.float32)
    step_row = conv_rows + in_rows
    squares = (
        total[step_row + 1 : step_row + 2]
        + total[step_row + 2 : step_row + 3]
        + total[step_row + 3 : step_row + 4]
    )
    scale = lax.rsqrt(squares / width + EPS)
    rounded = (total * scale).astype(jnp.bfloat16).astype(jnp.float32)
    fresh = rounded[:conv_rows]
    hist_wide[: taps - 2, :] = hist_ref[1:, :].astype(jnp.float32)
    for j in range(conv_rows):
        hist_wide[taps - 2 : taps - 1, j * LANES : (j + 1) * LANES] = fresh[j : j + 1]
    hist_out_ref[...] = hist_wide[...].astype(jnp.bfloat16)
    acc = hist_rows[pl.ds(0, conv_rows), :] * taps_rows[pl.ds(0, conv_rows), :]
    for k in range(1, taps - 1):
        part = pl.ds(k * conv_rows, conv_rows)
        acc += hist_rows[part, :] * taps_rows[part, :]
    acc += fresh * taps_rows[pl.ds((taps - 1) * conv_rows, conv_rows), :]
    conv = silu(acc)
    maps = conv[in_rows:]
    raw = rounded[step_row : step_row + 1, :heads] + bias_ref[...]
    step = jnp.maximum(raw, 0.0) + jnp.log1p(jnp.exp(-jnp.abs(raw)))
    decay = jnp.exp(-step * jnp.exp(rate_ref[...]))
    pad = jnp.zeros((LANES - in_rows, LANES), jnp.float32)
    columns = jnp.concatenate([conv[:in_rows], pad], axis=0).T
    per_row = LANES // head_dim
    per_group = heads // groups
    for g in range(groups):
        write = maps[g : g + 1]
        for h in range(g * per_group, (g + 1) * per_group):
            r, c = h // per_row, h % per_row
            column = columns[c * head_dim : (c + 1) * head_dim, r : r + 1] * step[:, h : h + 1]
            state_out_ref[h] = decay[:, h : h + 1] * state_ref[h] + column * write
        block = state_out_ref[g * per_group : (g + 1) * per_group].reshape(
            per_group * head_dim, state_dim
        )
        read = lax.dot_general(
            maps,
            block,
            ROW_ROW,
            precision=lax.Precision.HIGHEST,
            preferred_element_type=jnp.float32,
        )
        span = per_group * head_dim // LANES
        for j in range(span):
            read_rows[g * span + j : g * span + j + 1, :] = read[
                map_rows + g : map_rows + g + 1, j * LANES : (j + 1) * LANES
            ]
    gated = read_rows[...] * silu(rounded[conv_rows : conv_rows + in_rows])
    sums = jnp.sum(gated * gated, axis=1, keepdims=True)
    owner = lax.broadcasted_iota(jnp.int32, (in_rows, 1), 0) // (in_rows // groups)
    block_scale = jnp.zeros((in_rows, 1), jnp.float32)
    for g in range(groups):
        mine = owner == g
        mean = jnp.sum(jnp.where(mine, sums, 0.0), axis=0, keepdims=True) / (
            in_rows // groups * LANES
        )
        block_scale = jnp.where(mine, lax.rsqrt(mean + EPS), block_scale)
    normed = (gated * block_scale * ggain_ref[...]).astype(jnp.bfloat16)
    for k in range(ways):
        normed_ref[k] = normed


def mixer(width, groups, got, taps, hist, bias, rate, state, ggain):
    ways = got.shape[0]
    heads, head_dim, state_dim = state.shape
    in_rows = heads * head_dim // LANES
    conv_rows = in_rows + 2 * groups * state_dim // LANES
    return pl.pallas_call(
        functools.partial(mixer_kernel, width, groups),
        out_shape=[
            jax.ShapeDtypeStruct(state.shape, jnp.float32),
            jax.ShapeDtypeStruct(hist.shape, jnp.bfloat16),
            jax.ShapeDtypeStruct((ways, in_rows, LANES), jnp.bfloat16),
        ],
        in_specs=[VMEM_SPEC] * 7,
        out_specs=[VMEM_SPEC] * 3,
        scratch_shapes=[
            pltpu.VMEM((in_rows, LANES), jnp.float32),
            pltpu.VMEM((taps.shape[0] * conv_rows, LANES), jnp.float32),
            pltpu.VMEM((hist.shape[0] * conv_rows, LANES), jnp.float32),
            pltpu.VMEM(hist.shape, jnp.float32),
        ],
        compiler_params=params(8),
        cost_estimate=COST,
    )(got, taps, hist, bias, rate, state, ggain)


def output_kernel(got_ref, w_ref, first_ref, out_ref, stage):
    ways, slots, _ = got_ref.shape
    for k in range(ways):
        stage[pl.ds(k * slots, slots), :] = got_ref[k].astype(jnp.float32)
    rows = jnp.concatenate(
        [stage[pl.ds(j, ways, stride=slots), :].astype(jnp.bfloat16) for j in range(slots)], axis=1
    )
    mixed = jnp.dot(rows, w_ref[...], preferred_element_type=jnp.float32)
    second = (first_ref[...].astype(jnp.float32) + mixed).astype(jnp.bfloat16)
    for k in range(ways):
        out_ref[k] = second


def output(got, w, first):
    ways, slots, _ = got.shape
    return pl.pallas_call(
        output_kernel,
        out_shape=jax.ShapeDtypeStruct((ways,) + first.shape, jnp.bfloat16),
        in_specs=[VMEM_SPEC] * 3,
        out_specs=VMEM_SPEC,
        scratch_shapes=[pltpu.VMEM((ways * slots, LANES), jnp.float32)],
        compiler_params=params(4),
        cost_estimate=COST,
    )(got, w, first)


def final_kernel(got_ref, second_ref, out_ref):
    share = got_ref[0]
    for k in range(1, got_ref.shape[0]):
        share += got_ref[k]
    out_ref[...] = (second_ref[0].astype(jnp.float32) + 0.5 * share).astype(jnp.bfloat16)


def final(got, second_all):
    return pl.pallas_call(
        final_kernel,
        out_shape=jax.ShapeDtypeStruct(second_all.shape[1:], jnp.bfloat16),
        in_specs=[VMEM_SPEC] * 2,
        out_specs=VMEM_SPEC,
        compiler_params=params(2),
    )(got, second_all)


def fast_body(
    ways,
    tokens,
    first_gain,
    first_gate,
    first_up,
    first_down,
    mix_gain,
    w_input,
    w_outgate,
    w_write,
    w_read,
    w_step,
    conv_taps,
    conv_history,
    step_bias,
    rate_log,
    mixer_state,
    group_gain,
    w_output,
    second_gain,
    second_gate,
    second_up,
    second_down,
):
    width = first_gate.shape[0]
    _, heads, head_dim, state_dim = mixer_state.shape
    groups = w_write.shape[1] // state_dim
    conv_width = conv_taps.shape[1]
    used = (conv_width + heads * head_dim) // LANES + 4
    slots = -(-used // 16) * 16
    scope = jax.named_scope

    with scope("repeat"):
        blocks = repeat(tokens, ways)
    whole = exchange(blocks)
    with scope("ff1"):
        down1 = ff(whole, first_gain.reshape(1, width), first_gate.T, first_up.T, first_down)
    got1 = exchange(down1)
    with scope("project"):
        first, packed = project(
            got1, tokens, mix_gain.reshape(1, -1), w_input, w_write, w_read, w_outgate, w_step.T, slots
        )
    got2 = exchange(packed)
    with scope("mixer"):
        state_out, history_out, normed = mixer(
            width,
            groups,
            got2,
            conv_taps,
            conv_history[0],
            step_bias.reshape(1, heads),
            rate_log.reshape(1, heads),
            mixer_state[0],
            group_gain.reshape(-1, LANES),
        )
    got3 = exchange(normed)
    with scope("output"):
        second_all = output(got3, w_output, first)
    whole2 = exchange(second_all)
    with scope("ff2"):
        down2 = ff(whole2, second_gain.reshape(1, width), second_gate.T, second_up.T, second_down)
    got4 = exchange(down2)
    with scope("final"):
        layer_out = final(got4, second_all)
    return layer_out, state_out[None], history_out[None]


def friendly(ways, args):
    tokens, gate, taps, state, w_write = args[0], args[2], args[11], args[15], args[8]
    count, heads, head_dim, state_dim = state.shape
    return (
        count == 1
        and tokens.shape[0] == ways == 8
        and tokens.shape[1] % LANES == 0
        and gate.shape[1] % 64 == 0
        and taps.shape[1] % (8 * LANES) == 0
        and state_dim == LANES
        and LANES % head_dim == 0
        and heads < LANES
        and 2 * (w_write.shape[1] // state_dim) == 8
        and heads * head_dim % (16 * LANES) == 0
    )


def gather(block, ways):
    return exchange(jnp.broadcast_to(block[None], (ways,) + block.shape))


def scatter_sum(partial, ways):
    rows, width = partial.shape
    blocks = partial.reshape(rows, ways, width // ways).transpose(1, 0, 2)
    return jnp.sum(exchange(blocks), axis=0)


def half_block(resid, gain, w_gate, w_up, w_down, ways):
    rows = resid.shape[0]
    whole = gather(resid, ways).transpose(1, 0, 2).reshape(rows, -1)
    whole_f = whole.astype(jnp.float32)
    scale = lax.rsqrt(jnp.mean(whole_f * whole_f, axis=-1, keepdims=True) + EPS)
    normed = (whole_f * scale * gain).astype(jnp.bfloat16)
    gate = jnp.dot(normed, w_gate, preferred_element_type=jnp.float32)
    upper = jnp.dot(normed, w_up, preferred_element_type=jnp.float32)
    hidden = (jax.nn.silu(gate) * upper).astype(jnp.bfloat16)
    down = jnp.dot(hidden, w_down, preferred_element_type=jnp.float32)
    share = scatter_sum(down, ways)
    return (resid.astype(jnp.float32) + 0.5 * share).astype(jnp.bfloat16)


def make_plain(ways):
    def body(
        tokens,
        first_gain,
        first_gate,
        first_up,
        first_down,
        mix_gain,
        w_input,
        w_outgate,
        w_write,
        w_read,
        w_step,
        conv_taps,
        conv_history,
        step_bias,
        rate_log,
        mixer_state,
        group_gain,
        w_output,
        second_gain,
        second_gate,
        second_up,
        second_down,
    ):
        width = first_gate.shape[0]
        count = mixer_state.shape[0]
        heads = mixer_state.shape[1]
        head_dim = mixer_state.shape[2]
        state_dim = mixer_state.shape[3]
        ssd_width = heads * head_dim
        groups = w_write.shape[1] // state_dim
        per_group = heads // groups
        rows = tokens.shape[0]
        first = half_block(tokens, first_gain, first_gate, first_up, first_down, ways)
        first_f = first.astype(jnp.float32)
        squares = jnp.sum(first_f * first_f, axis=1, keepdims=True)
        premix = (first_f * mix_gain).astype(jnp.bfloat16)
        parts = [
            jnp.dot(premix, w, preferred_element_type=jnp.float32)
            for w in (w_input, w_write, w_read, w_outgate, w_step)
        ]
        ends = []
        total = 0
        for p in parts:
            total += p.shape[1]
            ends.append(total)
        padded = -(-(total + 1) // 1024) * 1024
        pad = jnp.zeros((rows, padded - total - 1), jnp.float32)
        packed = jnp.concatenate(parts + [squares, pad], axis=1)
        packed = packed.reshape(ways, count, padded)
        summed = jnp.sum(exchange(packed), axis=0)
        own_squares = summed[:, total : total + 1]
        scale = lax.rsqrt(own_squares / width + EPS)
        scaled = (scale * summed[:, :total]).astype(jnp.bfloat16)
        fresh = scaled[:, : ends[2]]
        outgate = scaled[:, ends[2] : ends[3]]
        steps_raw = scaled[:, ends[3] :]
        window = jnp.concatenate([conv_history, fresh[:, None, :]], axis=1)
        history_out = window[:, 1:]
        conv = jax.nn.silu(
            jnp.sum(window.astype(jnp.float32) * conv_taps.astype(jnp.float32)[None], axis=1)
        )
        conv_in = conv[:, :ssd_width].reshape(count, groups, per_group, head_dim)
        conv_write = conv[:, ssd_width : ssd_width + groups * state_dim].reshape(
            count, groups, state_dim
        )
        conv_read = conv[:, ssd_width + groups * state_dim :].reshape(count, groups, state_dim)
        step = jax.nn.softplus(steps_raw.astype(jnp.float32) + step_bias)
        decay = jnp.exp(-step * jnp.exp(rate_log))
        state = mixer_state.reshape(count, groups, per_group, head_dim, state_dim)
        decay_g = decay.reshape(count, groups, per_group)
        step_g = step.reshape(count, groups, per_group)
        written = (step_g[..., None] * conv_in)[..., None] * conv_write[:, :, None, None, :]
        new_state = decay_g[..., None, None] * state + written
        read_out = jnp.sum(new_state * conv_read[:, :, None, None, :], axis=-1)
        gated = read_out.reshape(count, ssd_width) * jax.nn.silu(outgate.astype(jnp.float32))
        blocks = gated.reshape(count, groups, ssd_width // groups)
        block_scale = lax.rsqrt(jnp.mean(blocks * blocks, axis=-1, keepdims=True) + EPS)
        normed = ((blocks * block_scale).reshape(count, ssd_width) * group_gain).astype(jnp.bfloat16)
        mixed = jnp.dot(
            gather(normed, ways).reshape(rows, ssd_width),
            w_output,
            preferred_element_type=jnp.float32,
        )
        second = (first_f + mixed).astype(jnp.bfloat16)
        layer_out = half_block(second, second_gain, second_gate, second_up, second_down, ways)
        state_out = new_state.reshape(count, heads, head_dim, state_dim)
        return (layer_out, state_out, history_out)

    return body


def solution(mesh):
    whole = P(AXES)
    rows = P(AXES, None)
    columns = P(None, AXES)
    own = ("dp",) + AXES
    ways = mesh.shape["kv"] * mesh.shape["tp"]
    plain = make_plain(ways)

    def body(*args):
        if friendly(ways, args):
            return fast_body(ways, *args)
        return plain(*args)

    return jax.shard_map(
        body,
        mesh=mesh,
        in_specs=(
            P("dp", AXES),
            P(),
            columns,
            columns,
            rows,
            whole,
            rows,
            rows,
            rows,
            rows,
            rows,
            P(),
            P(own, None, None),
            P(),
            P(),
            P(own, None, None, None),
            P(),
            columns,
            P(),
            columns,
            columns,
            rows,
        ),
        out_specs=(P("dp", AXES), P(own, None, None, None), P(own, None, None)),
        check_vma=False,
    )
```

```python
import functools

import jax
import jax.numpy as jnp
from jax import lax
from jax.experimental import pallas as pl
from jax.experimental.pallas import tpu as pltpu
from jax.sharding import PartitionSpec as P

EPS = 1e-06
AXES = ("kv", "tp")
LANES = 128
MIB = 1 << 20
VMEM_SPEC = pl.BlockSpec(memory_space=pltpu.VMEM)
ROW_ROW = (((1,), (1,)), ((), ()))


def exchange(blocks, order=None):
    groups = None if order is None else [list(order)]
    return lax.all_to_all(
        blocks, AXES, split_axis=0, concat_axis=0, tiled=True, axis_index_groups=groups
    )


def params(megabytes):
    return pltpu.CompilerParams(vmem_limit_bytes=megabytes * MIB)


COST = pl.CostEstimate(flops=10**10, bytes_accessed=1000, transcendentals=0)


def silu(x):
    return x / (1.0 + jnp.exp(-x))


def repeat_kernel(block_ref, out_ref):
    for k in range(out_ref.shape[0]):
        out_ref[k] = block_ref[...]


def repeat(block, ways):
    return pl.pallas_call(
        repeat_kernel,
        out_shape=jax.ShapeDtypeStruct((ways,) + block.shape, block.dtype),
        in_specs=[VMEM_SPEC],
        out_specs=VMEM_SPEC,
        compiler_params=params(2),
        cost_estimate=COST,
    )(block)


def ff_kernel(place, extras, x_ref, gain_ref, gate_ref, up_ref, down_ref, *refs):
    kept, out_ref, stored, sems = refs[:extras], refs[extras], refs[extras + 1 : -1], refs[-1]
    copies = [
        pltpu.make_async_copy(source, target, sems.at[i])
        for i, (source, target) in enumerate(zip(kept, stored))
    ]
    for copy in copies:
        copy.start()
    ways, rows, chan = x_ref.shape
    pieces = [x_ref[place[k]].astype(jnp.float32) for k in range(ways)]
    total = jnp.zeros((rows, 1), jnp.float32)
    for piece in pieces:
        total += jnp.sum(piece * piece, axis=1, keepdims=True)
    scale = lax.rsqrt(total / (ways * chan) + EPS)
    normed = jnp.concatenate(
        [
            (piece * scale * gain_ref[:, k * chan : (k + 1) * chan]).astype(jnp.bfloat16)
            for k, piece in enumerate(pieces)
        ],
        axis=1,
    )
    gate = lax.dot_general(normed, gate_ref[...], ROW_ROW, preferred_element_type=jnp.float32)
    upper = lax.dot_general(normed, up_ref[...], ROW_ROW, preferred_element_type=jnp.float32)
    hidden = (silu(gate) * upper).astype(jnp.bfloat16)
    down = jnp.dot(hidden, down_ref[...], preferred_element_type=jnp.float32)
    for k in range(ways):
        out_ref[place[k]] = down[:, k * chan : (k + 1) * chan].astype(jnp.bfloat16)
    for copy in copies:
        copy.wait()


def ff(place, whole, gain, gate, up, down, *kept):
    return pl.pallas_call(
        functools.partial(ff_kernel, place, len(kept)),
        out_shape=[jax.ShapeDtypeStruct(whole.shape, jnp.bfloat16)]
        + [jax.ShapeDtypeStruct(k.shape, k.dtype) for k in kept],
        in_specs=[VMEM_SPEC] * (5 + len(kept)),
        out_specs=[VMEM_SPEC] + [pl.BlockSpec(memory_space=pltpu.HBM)] * len(kept),
        scratch_shapes=[pltpu.SemaphoreType.DMA((max(1, len(kept)),))],
        compiler_params=params(8),
        cost_estimate=COST,
    )(whole, gain, gate, up, down, *kept)


def project_kernel(place, got_ref, tok_ref, gain_ref, win_ref, wwrite_ref, wread_ref, wgate_ref, wstep_ref,
                   first_ref, out_ref, stage):
    ways, rows, chan = got_ref.shape
    slots = out_ref.shape[1]
    share = got_ref[0].astype(jnp.float32)
    for k in range(1, ways):
        share += got_ref[k].astype(jnp.float32)
    first = (tok_ref[...].astype(jnp.float32) + 0.5 * share).astype(jnp.bfloat16)
    first_ref[...] = first
    first_f = first.astype(jnp.float32)
    squares = jnp.sum(first_f * first_f, axis=1, keepdims=True)
    premix = (first_f * gain_ref[...]).astype(jnp.bfloat16)
    row = 0
    for w_ref in (win_ref, wwrite_ref, wread_ref, wgate_ref):
        part = jnp.dot(premix, w_ref[...], preferred_element_type=jnp.float32)
        for j in range(part.shape[1] // LANES):
            stage[pl.ds(row, rows, stride=slots), :] = part[:, j * LANES : (j + 1) * LANES]
            row += 1
    steps = lax.dot_general(premix, wstep_ref[...], ROW_ROW, preferred_element_type=jnp.float32)
    stage[pl.ds(row, rows, stride=slots), :] = jnp.zeros((rows, LANES), jnp.float32)
    stage[pl.ds(row, rows, stride=slots), : steps.shape[1]] = steps
    row += 1
    rest = jnp.broadcast_to(squares, (rows, LANES))
    for _ in range(3):
        term = rest.astype(jnp.bfloat16).astype(jnp.float32)
        stage[pl.ds(row, rows, stride=slots), :] = term
        rest = rest - term
        row += 1
    for j in range(row, slots):
        stage[pl.ds(j, rows, stride=slots), :] = jnp.zeros((rows, LANES), jnp.float32)
    for s in range(rows):
        out_ref[place[s]] = stage[pl.ds(s * slots, slots), :].astype(jnp.bfloat16)


def project(place, got, tokens, gain, w_in, w_write, w_read, w_gate, w_step, slots):
    ways, rows, chan = got.shape
    return pl.pallas_call(
        functools.partial(project_kernel, place),
        out_shape=[
            jax.ShapeDtypeStruct((rows, chan), jnp.bfloat16),
            jax.ShapeDtypeStruct((rows, slots, LANES), jnp.bfloat16),
        ],
        in_specs=[VMEM_SPEC] * 8,
        out_specs=[VMEM_SPEC] * 2,
        scratch_shapes=[pltpu.VMEM((rows * slots, LANES), jnp.float32)],
        compiler_params=params(8),
        cost_estimate=COST,
    )(got, tokens, gain, w_in, w_write, w_read, w_gate, w_step)


def mixer_kernel(width, groups, got_ref, taps_ref, hist_ref, bias_ref, rate_ref, state_ref, ggain_ref,
                 state_out_ref, hist_out_ref, normed_ref, read_rows, taps_rows, hist_rows, hist_wide):
    ways = got_ref.shape[0]
    heads, head_dim, state_dim = state_ref.shape
    in_rows = heads * head_dim // LANES
    map_rows = groups * state_dim // LANES
    conv_rows = in_rows + 2 * map_rows
    taps = taps_ref.shape[0]
    for j in range(conv_rows):
        part = pl.ds(j * LANES, LANES)
        taps_rows[pl.ds(j, taps, stride=conv_rows), :] = taps_ref[:, part].astype(jnp.float32)
        hist_rows[pl.ds(j, taps - 1, stride=conv_rows), :] = hist_ref[:, part].astype(jnp.float32)
    total = got_ref[0].astype(jnp.float32)
    for k in range(1, ways):
        total += got_ref[k].astype(jnp.float32)
    step_row = conv_rows + in_rows
    squares = (
        total[step_row + 1 : step_row + 2]
        + total[step_row + 2 : step_row + 3]
        + total[step_row + 3 : step_row + 4]
    )
    scale = lax.rsqrt(squares / width + EPS)
    rounded = (total * scale).astype(jnp.bfloat16).astype(jnp.float32)
    fresh = rounded[:conv_rows]
    hist_wide[: taps - 2, :] = hist_ref[1:, :].astype(jnp.float32)
    for j in range(conv_rows):
        hist_wide[taps - 2 : taps - 1, j * LANES : (j + 1) * LANES] = fresh[j : j + 1]
    hist_out_ref[...] = hist_wide[...].astype(jnp.bfloat16)
    acc = hist_rows[pl.ds(0, conv_rows), :] * taps_rows[pl.ds(0, conv_rows), :]
    for k in range(1, taps - 1):
        part = pl.ds(k * conv_rows, conv_rows)
        acc += hist_rows[part, :] * taps_rows[part, :]
    acc += fresh * taps_rows[pl.ds((taps - 1) * conv_rows, conv_rows), :]
    conv = silu(acc)
    maps = conv[in_rows:]
    raw = rounded[step_row : step_row + 1, :heads] + bias_ref[...]
    step = jnp.maximum(raw, 0.0) + jnp.log1p(jnp.exp(-jnp.abs(raw)))
    decay = jnp.exp(-step * jnp.exp(rate_ref[...]))
    pad = jnp.zeros((LANES - in_rows, LANES), jnp.float32)
    columns = jnp.concatenate([conv[:in_rows], pad], axis=0).T
    per_row = LANES // head_dim
    per_group = heads // groups
    for g in range(groups):
        write = maps[g : g + 1]
        for h in range(g * per_group, (g + 1) * per_group):
            r, c = h // per_row, h % per_row
            column = columns[c * head_dim : (c + 1) * head_dim, r : r + 1] * step[:, h : h + 1]
            state_out_ref[h] = decay[:, h : h + 1] * state_ref[h] + column * write
        block = state_out_ref[g * per_group : (g + 1) * per_group].reshape(
            per_group * head_dim, state_dim
        )
        read = lax.dot_general(
            maps,
            block,
            ROW_ROW,
            precision=lax.Precision.HIGHEST,
            preferred_element_type=jnp.float32,
        )
        span = per_group * head_dim // LANES
        for j in range(span):
            read_rows[g * span + j : g * span + j + 1, :] = read[
                map_rows + g : map_rows + g + 1, j * LANES : (j + 1) * LANES
            ]
    gated = read_rows[...] * silu(rounded[conv_rows : conv_rows + in_rows])
    sums = jnp.sum(gated * gated, axis=1, keepdims=True)
    owner = lax.broadcasted_iota(jnp.int32, (in_rows, 1), 0) // (in_rows // groups)
    block_scale = jnp.zeros((in_rows, 1), jnp.float32)
    for g in range(groups):
        mine = owner == g
        mean = jnp.sum(jnp.where(mine, sums, 0.0), axis=0, keepdims=True) / (
            in_rows // groups * LANES
        )
        block_scale = jnp.where(mine, lax.rsqrt(mean + EPS), block_scale)
    normed = (gated * block_scale * ggain_ref[...]).astype(jnp.bfloat16)
    for k in range(ways):
        normed_ref[k] = normed


def mixer(width, groups, got, taps, hist, bias, rate, state, ggain):
    ways = got.shape[0]
    heads, head_dim, state_dim = state.shape
    in_rows = heads * head_dim // LANES
    conv_rows = in_rows + 2 * groups * state_dim // LANES
    return pl.pallas_call(
        functools.partial(mixer_kernel, width, groups),
        out_shape=[
            pltpu.VMEM(state.shape, jnp.float32),
            pltpu.VMEM(hist.shape, jnp.bfloat16),
            jax.ShapeDtypeStruct((ways, in_rows, LANES), jnp.bfloat16),
        ],
        in_specs=[VMEM_SPEC] * 7,
        out_specs=[VMEM_SPEC] * 3,
        scratch_shapes=[
            pltpu.VMEM((in_rows, LANES), jnp.float32),
            pltpu.VMEM((taps.shape[0] * conv_rows, LANES), jnp.float32),
            pltpu.VMEM((hist.shape[0] * conv_rows, LANES), jnp.float32),
            pltpu.VMEM(hist.shape, jnp.float32),
        ],
        compiler_params=params(8),
        cost_estimate=COST,
    )(got, taps, hist, bias, rate, state, ggain)


def output_kernel(place, got_ref, w_ref, first_ref, out_ref, stage):
    ways, slots, _ = got_ref.shape
    for k in range(ways):
        stage[pl.ds(k * slots, slots), :] = got_ref[place[k]].astype(jnp.float32)
    rows = jnp.concatenate(
        [stage[pl.ds(j, ways, stride=slots), :].astype(jnp.bfloat16) for j in range(slots)], axis=1
    )
    mixed = jnp.dot(rows, w_ref[...], preferred_element_type=jnp.float32)
    second = (first_ref[...].astype(jnp.float32) + mixed).astype(jnp.bfloat16)
    for k in range(ways):
        out_ref[k] = second


def output(place, got, w, first):
    ways, slots, _ = got.shape
    return pl.pallas_call(
        functools.partial(output_kernel, place),
        out_shape=jax.ShapeDtypeStruct((ways,) + first.shape, jnp.bfloat16),
        in_specs=[VMEM_SPEC] * 3,
        out_specs=VMEM_SPEC,
        scratch_shapes=[pltpu.VMEM((ways * slots, LANES), jnp.float32)],
        compiler_params=params(4),
        cost_estimate=COST,
    )(got, w, first)


def final_kernel(got_ref, second_ref, out_ref):
    share = got_ref[0].astype(jnp.float32)
    for k in range(1, got_ref.shape[0]):
        share += got_ref[k].astype(jnp.float32)
    out_ref[...] = (second_ref[0].astype(jnp.float32) + 0.5 * share).astype(jnp.bfloat16)


def final(got, second_all):
    return pl.pallas_call(
        final_kernel,
        out_shape=jax.ShapeDtypeStruct(second_all.shape[1:], jnp.bfloat16),
        in_specs=[VMEM_SPEC] * 2,
        out_specs=VMEM_SPEC,
        compiler_params=params(2),
    )(got, second_all)


def fast_body(
    ways,
    leader,
    tokens,
    first_gain,
    first_gate,
    first_up,
    first_down,
    mix_gain,
    w_input,
    w_outgate,
    w_write,
    w_read,
    w_step,
    conv_taps,
    conv_history,
    step_bias,
    rate_log,
    mixer_state,
    group_gain,
    w_output,
    second_gain,
    second_gate,
    second_up,
    second_down,
):
    width = first_gate.shape[0]
    _, heads, head_dim, state_dim = mixer_state.shape
    groups = w_write.shape[1] // state_dim
    conv_width = conv_taps.shape[1]
    used = (conv_width + heads * head_dim) // LANES + 4
    slots = -(-used // 16) * 16
    scope = jax.named_scope
    order = (leader,) + tuple(k for k in range(ways) if k != leader)
    place = tuple(order.index(k) for k in range(ways))

    with scope("repeat"):
        blocks = repeat(tokens, ways)
    whole = exchange(blocks, order)
    with scope("ff1"):
        (down1,) = ff(place, whole, first_gain.reshape(1, width), first_gate.T, first_up.T, first_down)
    got1 = exchange(down1, order)
    with scope("project"):
        first, packed = project(
            place,
            got1, tokens, mix_gain.reshape(1, -1), w_input, w_write, w_read, w_outgate, w_step.T, slots
        )
    got2 = exchange(packed, order)
    with scope("mixer"):
        new_state, new_hist, normed = mixer(
            width,
            groups,
            got2,
            conv_taps,
            conv_history[0],
            step_bias.reshape(1, heads),
            rate_log.reshape(1, heads),
            mixer_state[0],
            group_gain.reshape(-1, LANES),
        )
    got3 = exchange(normed, order)
    with scope("output"):
        second_all = output(place, got3, w_output, first)
    whole2 = exchange(second_all, order)
    with scope("ff2"):
        down2, state_out, history_out = ff(
            place,
            whole2,
            second_gain.reshape(1, width),
            second_gate.T,
            second_up.T,
            second_down,
            new_state,
            new_hist,
        )
    got4 = exchange(down2, order)
    with scope("final"):
        layer_out = final(got4, second_all)
    return layer_out, state_out[None], history_out[None]


def friendly(ways, args):
    tokens, gate, taps, state, w_write = args[0], args[2], args[11], args[15], args[8]
    count, heads, head_dim, state_dim = state.shape
    return (
        count == 1
        and tokens.shape[0] == ways == 8
        and tokens.shape[1] % LANES == 0
        and gate.shape[1] % 64 == 0
        and taps.shape[1] % (8 * LANES) == 0
        and state_dim == LANES
        and LANES % head_dim == 0
        and heads < LANES
        and 2 * (w_write.shape[1] // state_dim) == 8
        and heads * head_dim % (16 * LANES) == 0
    )


def gather(block, ways):
    return exchange(jnp.broadcast_to(block[None], (ways,) + block.shape))


def scatter_sum(partial, ways):
    rows, width = partial.shape
    blocks = partial.reshape(rows, ways, width // ways).transpose(1, 0, 2)
    return jnp.sum(exchange(blocks), axis=0)


def half_block(resid, gain, w_gate, w_up, w_down, ways):
    rows = resid.shape[0]
    whole = gather(resid, ways).transpose(1, 0, 2).reshape(rows, -1)
    whole_f = whole.astype(jnp.float32)
    scale = lax.rsqrt(jnp.mean(whole_f * whole_f, axis=-1, keepdims=True) + EPS)
    normed = (whole_f * scale * gain).astype(jnp.bfloat16)
    gate = jnp.dot(normed, w_gate, preferred_element_type=jnp.float32)
    upper = jnp.dot(normed, w_up, preferred_element_type=jnp.float32)
    hidden = (jax.nn.silu(gate) * upper).astype(jnp.bfloat16)
    down = jnp.dot(hidden, w_down, preferred_element_type=jnp.float32)
    share = scatter_sum(down, ways)
    return (resid.astype(jnp.float32) + 0.5 * share).astype(jnp.bfloat16)


def make_plain(ways):
    def body(
        tokens,
        first_gain,
        first_gate,
        first_up,
        first_down,
        mix_gain,
        w_input,
        w_outgate,
        w_write,
        w_read,
        w_step,
        conv_taps,
        conv_history,
        step_bias,
        rate_log,
        mixer_state,
        group_gain,
        w_output,
        second_gain,
        second_gate,
        second_up,
        second_down,
    ):
        width = first_gate.shape[0]
        count = mixer_state.shape[0]
        heads = mixer_state.shape[1]
        head_dim = mixer_state.shape[2]
        state_dim = mixer_state.shape[3]
        ssd_width = heads * head_dim
        groups = w_write.shape[1] // state_dim
        per_group = heads // groups
        rows = tokens.shape[0]
        first = half_block(tokens, first_gain, first_gate, first_up, first_down, ways)
        first_f = first.astype(jnp.float32)
        squares = jnp.sum(first_f * first_f, axis=1, keepdims=True)
        premix = (first_f * mix_gain).astype(jnp.bfloat16)
        parts = [
            jnp.dot(premix, w, preferred_element_type=jnp.float32)
            for w in (w_input, w_write, w_read, w_outgate, w_step)
        ]
        ends = []
        total = 0
        for p in parts:
            total += p.shape[1]
            ends.append(total)
        padded = -(-(total + 1) // 1024) * 1024
        pad = jnp.zeros((rows, padded - total - 1), jnp.float32)
        packed = jnp.concatenate(parts + [squares, pad], axis=1)
        packed = packed.reshape(ways, count, padded)
        summed = jnp.sum(exchange(packed), axis=0)
        own_squares = summed[:, total : total + 1]
        scale = lax.rsqrt(own_squares / width + EPS)
        scaled = (scale * summed[:, :total]).astype(jnp.bfloat16)
        fresh = scaled[:, : ends[2]]
        outgate = scaled[:, ends[2] : ends[3]]
        steps_raw = scaled[:, ends[3] :]
        window = jnp.concatenate([conv_history, fresh[:, None, :]], axis=1)
        history_out = window[:, 1:]
        conv = jax.nn.silu(
            jnp.sum(window.astype(jnp.float32) * conv_taps.astype(jnp.float32)[None], axis=1)
        )
        conv_in = conv[:, :ssd_width].reshape(count, groups, per_group, head_dim)
        conv_write = conv[:, ssd_width : ssd_width + groups * state_dim].reshape(
            count, groups, state_dim
        )
        conv_read = conv[:, ssd_width + groups * state_dim :].reshape(count, groups, state_dim)
        step = jax.nn.softplus(steps_raw.astype(jnp.float32) + step_bias)
        decay = jnp.exp(-step * jnp.exp(rate_log))
        state = mixer_state.reshape(count, groups, per_group, head_dim, state_dim)
        decay_g = decay.reshape(count, groups, per_group)
        step_g = step.reshape(count, groups, per_group)
        written = (step_g[..., None] * conv_in)[..., None] * conv_write[:, :, None, None, :]
        new_state = decay_g[..., None, None] * state + written
        read_out = jnp.sum(new_state * conv_read[:, :, None, None, :], axis=-1)
        gated = read_out.reshape(count, ssd_width) * jax.nn.silu(outgate.astype(jnp.float32))
        blocks = gated.reshape(count, groups, ssd_width // groups)
        block_scale = lax.rsqrt(jnp.mean(blocks * blocks, axis=-1, keepdims=True) + EPS)
        normed = ((blocks * block_scale).reshape(count, ssd_width) * group_gain).astype(jnp.bfloat16)
        mixed = jnp.dot(
            gather(normed, ways).reshape(rows, ssd_width),
            w_output,
            preferred_element_type=jnp.float32,
        )
        second = (first_f + mixed).astype(jnp.bfloat16)
        layer_out = half_block(second, second_gain, second_gate, second_up, second_down, ways)
        state_out = new_state.reshape(count, heads, head_dim, state_dim)
        return (layer_out, state_out, history_out)

    return body


def solution(mesh):
    whole = P(AXES)
    rows = P(AXES, None)
    columns = P(None, AXES)
    own = ("dp",) + AXES
    kv, tp = mesh.shape["kv"], mesh.shape["tp"]
    ways = kv * tp
    leader = kv // 2 * tp + tp - 1
    plain = make_plain(ways)

    def body(*args):
        if friendly(ways, args):
            return fast_body(ways, leader, *args)
        return plain(*args)

    return jax.shard_map(
        body,
        mesh=mesh,
        in_specs=(
            P("dp", AXES),
            P(),
            columns,
            columns,
            rows,
            whole,
            rows,
            rows,
            rows,
            rows,
            rows,
            P(),
            P(own, None, None),
            P(),
            P(),
            P(own, None, None, None),
            P(),
            columns,
            P(),
            columns,
            columns,
            rows,
        ),
        out_specs=(P("dp", AXES), P(own, None, None, None), P(own, None, None)),
        check_vma=False,
    )
```

```python
import functools

import jax
import jax.numpy as jnp
from jax import lax
from jax.experimental import pallas as pl
from jax.experimental.pallas import tpu as pltpu
from jax.sharding import PartitionSpec as P

EPS = 1e-06
AXES = ("kv", "tp")
LANES = 128
MIB = 1 << 20
VMEM_SPEC = pl.BlockSpec(memory_space=pltpu.VMEM)
ROW_ROW = (((1,), (1,)), ((), ()))


def exchange(blocks, order=None):
    groups = None if order is None else [list(order)]
    return lax.all_to_all(
        blocks, AXES, split_axis=0, concat_axis=0, tiled=True, axis_index_groups=groups
    )


def params(megabytes):
    return pltpu.CompilerParams(vmem_limit_bytes=megabytes * MIB)


COST = pl.CostEstimate(flops=10**10, bytes_accessed=1000, transcendentals=0)


def silu(x):
    return x / (1.0 + jnp.exp(-x))


def repeat_kernel(block_ref, out_ref):
    for k in range(out_ref.shape[0]):
        out_ref[k] = block_ref[...]


def repeat(block, ways):
    return pl.pallas_call(
        repeat_kernel,
        out_shape=jax.ShapeDtypeStruct((ways,) + block.shape, block.dtype),
        in_specs=[VMEM_SPEC],
        out_specs=VMEM_SPEC,
        compiler_params=params(2),
        cost_estimate=COST,
    )(block)


def ff_kernel(place, extras, x_ref, gain_ref, gate_ref, up_ref, down_ref, *refs):
    kept, out_ref, stored, sems = refs[:extras], refs[extras], refs[extras + 1 : -1], refs[-1]
    copies = [
        pltpu.make_async_copy(source, target, sems.at[i])
        for i, (source, target) in enumerate(zip(kept, stored))
    ]
    for copy in copies:
        copy.start()
    ways, rows, chan = x_ref.shape
    pieces = [x_ref[place[k]].astype(jnp.float32) for k in range(ways)]
    total = jnp.zeros((rows, 1), jnp.float32)
    for piece in pieces:
        total += jnp.sum(piece * piece, axis=1, keepdims=True)
    scale = lax.rsqrt(total / (ways * chan) + EPS)
    normed = jnp.concatenate(
        [
            (piece * scale * gain_ref[:, k * chan : (k + 1) * chan]).astype(jnp.bfloat16)
            for k, piece in enumerate(pieces)
        ],
        axis=1,
    )
    gate = lax.dot_general(normed, gate_ref[...], ROW_ROW, preferred_element_type=jnp.float32)
    upper = lax.dot_general(normed, up_ref[...], ROW_ROW, preferred_element_type=jnp.float32)
    hidden = (silu(gate) * upper).astype(jnp.bfloat16)
    down = jnp.dot(hidden, down_ref[...], preferred_element_type=jnp.float32)
    for k in range(ways):
        out_ref[place[k]] = down[:, k * chan : (k + 1) * chan].astype(jnp.bfloat16)
    for copy in copies:
        copy.wait()


def ff(place, whole, gain, gate, up, down, *kept):
    return pl.pallas_call(
        functools.partial(ff_kernel, place, len(kept)),
        out_shape=[jax.ShapeDtypeStruct(whole.shape, jnp.bfloat16)]
        + [jax.ShapeDtypeStruct(k.shape, k.dtype) for k in kept],
        in_specs=[VMEM_SPEC] * (5 + len(kept)),
        out_specs=[VMEM_SPEC] + [pl.BlockSpec(memory_space=pltpu.HBM)] * len(kept),
        scratch_shapes=[pltpu.SemaphoreType.DMA((max(1, len(kept)),))],
        compiler_params=params(8),
        cost_estimate=COST,
    )(whole, gain, gate, up, down, *kept)


def project_kernel(place, got_ref, tok_ref, gain_ref, win_ref, wwrite_ref, wread_ref, wgate_ref, wstep_ref,
                   first_ref, out_ref, stage):
    ways, rows, chan = got_ref.shape
    slots = out_ref.shape[1]
    share = got_ref[0].astype(jnp.float32)
    for k in range(1, ways):
        share += got_ref[k].astype(jnp.float32)
    first = (tok_ref[...].astype(jnp.float32) + 0.5 * share).astype(jnp.bfloat16)
    first_ref[...] = first
    first_f = first.astype(jnp.float32)
    squares = jnp.sum(first_f * first_f, axis=1, keepdims=True)
    premix = (first_f * gain_ref[...]).astype(jnp.bfloat16)
    row = 0
    for w_ref in (win_ref, wwrite_ref, wread_ref, wgate_ref):
        part = jnp.dot(premix, w_ref[...], preferred_element_type=jnp.float32)
        for j in range(part.shape[1] // LANES):
            stage[pl.ds(row, rows, stride=slots), :] = part[:, j * LANES : (j + 1) * LANES]
            row += 1
    steps = lax.dot_general(premix, wstep_ref[...], ROW_ROW, preferred_element_type=jnp.float32)
    stage[pl.ds(row, rows, stride=slots), :] = jnp.zeros((rows, LANES), jnp.float32)
    stage[pl.ds(row, rows, stride=slots), : steps.shape[1]] = steps
    row += 1
    rest = jnp.broadcast_to(squares, (rows, LANES))
    for _ in range(3):
        term = rest.astype(jnp.bfloat16).astype(jnp.float32)
        stage[pl.ds(row, rows, stride=slots), :] = term
        rest = rest - term
        row += 1
    for j in range(row, slots):
        stage[pl.ds(j, rows, stride=slots), :] = jnp.zeros((rows, LANES), jnp.float32)
    for s in range(rows):
        out_ref[place[s]] = stage[pl.ds(s * slots, slots), :].astype(jnp.bfloat16)


def project(place, got, tokens, gain, w_in, w_write, w_read, w_gate, w_step, slots):
    ways, rows, chan = got.shape
    return pl.pallas_call(
        functools.partial(project_kernel, place),
        out_shape=[
            jax.ShapeDtypeStruct((rows, chan), jnp.bfloat16),
            jax.ShapeDtypeStruct((rows, slots, LANES), jnp.bfloat16),
        ],
        in_specs=[VMEM_SPEC] * 8,
        out_specs=[VMEM_SPEC] * 2,
        scratch_shapes=[pltpu.VMEM((rows * slots, LANES), jnp.float32)],
        compiler_params=params(8),
        cost_estimate=COST,
    )(got, tokens, gain, w_in, w_write, w_read, w_gate, w_step)


def mixer_kernel(width, groups, got_ref, taps_ref, hist_ref, bias_ref, rate_ref, state_ref, ggain_ref,
                 state_out_ref, hist_out_ref, normed_ref, read_rows, taps_rows, hist_rows, hist_wide):
    ways = got_ref.shape[0]
    heads, head_dim, state_dim = state_ref.shape
    in_rows = heads * head_dim // LANES
    map_rows = groups * state_dim // LANES
    conv_rows = in_rows + 2 * map_rows
    taps = taps_ref.shape[0]
    for j in range(conv_rows):
        part = pl.ds(j * LANES, LANES)
        taps_rows[pl.ds(j, taps, stride=conv_rows), :] = taps_ref[:, part].astype(jnp.float32)
        hist_rows[pl.ds(j, taps - 1, stride=conv_rows), :] = hist_ref[:, part].astype(jnp.float32)
    total = got_ref[0].astype(jnp.float32)
    for k in range(1, ways):
        total += got_ref[k].astype(jnp.float32)
    step_row = conv_rows + in_rows
    squares = (
        total[step_row + 1 : step_row + 2]
        + total[step_row + 2 : step_row + 3]
        + total[step_row + 3 : step_row + 4]
    )
    scale = lax.rsqrt(squares / width + EPS)
    rounded = (total * scale).astype(jnp.bfloat16).astype(jnp.float32)
    fresh = rounded[:conv_rows]
    hist_wide[: taps - 2, :] = hist_ref[1:, :].astype(jnp.float32)
    for j in range(conv_rows):
        hist_wide[taps - 2 : taps - 1, j * LANES : (j + 1) * LANES] = fresh[j : j + 1]
    hist_out_ref[...] = hist_wide[...].astype(jnp.bfloat16)
    acc = hist_rows[pl.ds(0, conv_rows), :] * taps_rows[pl.ds(0, conv_rows), :]
    for k in range(1, taps - 1):
        part = pl.ds(k * conv_rows, conv_rows)
        acc += hist_rows[part, :] * taps_rows[part, :]
    acc += fresh * taps_rows[pl.ds((taps - 1) * conv_rows, conv_rows), :]
    conv = silu(acc)
    maps = conv[in_rows:]
    raw = rounded[step_row : step_row + 1, :heads] + bias_ref[...]
    step = jnp.maximum(raw, 0.0) + jnp.log1p(jnp.exp(-jnp.abs(raw)))
    decay = jnp.exp(-step * jnp.exp(rate_ref[...]))
    maps_high = maps.astype(jnp.bfloat16)
    maps_low = (maps - maps_high.astype(jnp.float32)).astype(jnp.bfloat16)
    maps2 = jnp.concatenate([maps_high, maps_low], axis=0)
    pad = jnp.zeros((LANES - in_rows, LANES), jnp.float32)
    columns = jnp.concatenate([conv[:in_rows], pad], axis=0).T
    per_row = LANES // head_dim
    per_group = heads // groups
    for g in range(groups):
        write = maps[g : g + 1]
        for h in range(g * per_group, (g + 1) * per_group):
            r, c = h // per_row, h % per_row
            column = columns[c * head_dim : (c + 1) * head_dim, r : r + 1] * step[:, h : h + 1]
            state_out_ref[h] = decay[:, h : h + 1] * state_ref[h] + column * write
        block = state_out_ref[g * per_group : (g + 1) * per_group].reshape(
            per_group * head_dim, state_dim
        )
        high = block.astype(jnp.bfloat16)
        read = lax.dot_general(maps2, high, ROW_ROW, preferred_element_type=jnp.float32)
        low = (block - high.astype(jnp.float32)).astype(jnp.bfloat16)
        read += lax.dot_general(maps2, low, ROW_ROW, preferred_element_type=jnp.float32)
        count = 2 * map_rows
        read = read[:count] + read[count:]
        span = per_group * head_dim // LANES
        for j in range(span):
            read_rows[g * span + j : g * span + j + 1, :] = read[
                map_rows + g : map_rows + g + 1, j * LANES : (j + 1) * LANES
            ]
    gated = read_rows[...] * silu(rounded[conv_rows : conv_rows + in_rows])
    sums = jnp.sum(gated * gated, axis=1, keepdims=True)
    owner = lax.broadcasted_iota(jnp.int32, (in_rows, 1), 0) // (in_rows // groups)
    block_scale = jnp.zeros((in_rows, 1), jnp.float32)
    for g in range(groups):
        mine = owner == g
        mean = jnp.sum(jnp.where(mine, sums, 0.0), axis=0, keepdims=True) / (
            in_rows // groups * LANES
        )
        block_scale = jnp.where(mine, lax.rsqrt(mean + EPS), block_scale)
    normed = (gated * block_scale * ggain_ref[...]).astype(jnp.bfloat16)
    for k in range(ways):
        normed_ref[k] = normed


def mixer(width, groups, got, taps, hist, bias, rate, state, ggain):
    ways = got.shape[0]
    heads, head_dim, state_dim = state.shape
    in_rows = heads * head_dim // LANES
    conv_rows = in_rows + 2 * groups * state_dim // LANES
    return pl.pallas_call(
        functools.partial(mixer_kernel, width, groups),
        out_shape=[
            pltpu.VMEM(state.shape, jnp.float32),
            pltpu.VMEM(hist.shape, jnp.bfloat16),
            jax.ShapeDtypeStruct((ways, in_rows, LANES), jnp.bfloat16),
        ],
        in_specs=[VMEM_SPEC] * 7,
        out_specs=[VMEM_SPEC] * 3,
        scratch_shapes=[
            pltpu.VMEM((in_rows, LANES), jnp.float32),
            pltpu.VMEM((taps.shape[0] * conv_rows, LANES), jnp.float32),
            pltpu.VMEM((hist.shape[0] * conv_rows, LANES), jnp.float32),
            pltpu.VMEM(hist.shape, jnp.float32),
        ],
        compiler_params=params(8),
        cost_estimate=COST,
    )(got, taps, hist, bias, rate, state, ggain)


def output_kernel(place, got_ref, w_ref, first_ref, out_ref, stage):
    ways, slots, _ = got_ref.shape
    for k in range(ways):
        stage[pl.ds(k * slots, slots), :] = got_ref[place[k]].astype(jnp.float32)
    rows = jnp.concatenate(
        [stage[pl.ds(j, ways, stride=slots), :].astype(jnp.bfloat16) for j in range(slots)], axis=1
    )
    mixed = jnp.dot(rows, w_ref[...], preferred_element_type=jnp.float32)
    second = (first_ref[...].astype(jnp.float32) + mixed).astype(jnp.bfloat16)
    for k in range(ways):
        out_ref[k] = second


def output(place, got, w, first):
    ways, slots, _ = got.shape
    return pl.pallas_call(
        functools.partial(output_kernel, place),
        out_shape=jax.ShapeDtypeStruct((ways,) + first.shape, jnp.bfloat16),
        in_specs=[VMEM_SPEC] * 3,
        out_specs=VMEM_SPEC,
        scratch_shapes=[pltpu.VMEM((ways * slots, LANES), jnp.float32)],
        compiler_params=params(4),
        cost_estimate=COST,
    )(got, w, first)


def final_kernel(got_ref, second_ref, out_ref):
    share = got_ref[0].astype(jnp.float32)
    for k in range(1, got_ref.shape[0]):
        share += got_ref[k].astype(jnp.float32)
    out_ref[...] = (second_ref[0].astype(jnp.float32) + 0.5 * share).astype(jnp.bfloat16)


def final(got, second_all):
    return pl.pallas_call(
        final_kernel,
        out_shape=jax.ShapeDtypeStruct(second_all.shape[1:], jnp.bfloat16),
        in_specs=[VMEM_SPEC] * 2,
        out_specs=VMEM_SPEC,
        compiler_params=params(2),
    )(got, second_all)


def fast_body(
    ways,
    leader,
    tokens,
    first_gain,
    first_gate,
    first_up,
    first_down,
    mix_gain,
    w_input,
    w_outgate,
    w_write,
    w_read,
    w_step,
    conv_taps,
    conv_history,
    step_bias,
    rate_log,
    mixer_state,
    group_gain,
    w_output,
    second_gain,
    second_gate,
    second_up,
    second_down,
):
    width = first_gate.shape[0]
    _, heads, head_dim, state_dim = mixer_state.shape
    groups = w_write.shape[1] // state_dim
    conv_width = conv_taps.shape[1]
    used = (conv_width + heads * head_dim) // LANES + 4
    slots = -(-used // 16) * 16
    scope = jax.named_scope
    rest = [k for k in range(ways) if k != leader]
    rest[3], rest[4] = rest[4], rest[3]
    rest[-2], rest[-1] = rest[-1], rest[-2]
    order = (leader, *rest)
    place = tuple(order.index(k) for k in range(ways))

    with scope("repeat"):
        blocks = repeat(tokens, ways)
    whole = exchange(blocks, order)
    with scope("ff1"):
        (down1,) = ff(place, whole, first_gain.reshape(1, width), first_gate.T, first_up.T, first_down)
    got1 = exchange(down1, order)
    with scope("project"):
        first, packed = project(
            place,
            got1, tokens, mix_gain.reshape(1, -1), w_input, w_write, w_read, w_outgate, w_step.T, slots
        )
    got2 = exchange(packed, order)
    with scope("mixer"):
        new_state, new_hist, normed = mixer(
            width,
            groups,
            got2,
            conv_taps,
            conv_history[0],
            step_bias.reshape(1, heads),
            rate_log.reshape(1, heads),
            mixer_state[0],
            group_gain.reshape(-1, LANES),
        )
    got3 = exchange(normed, order)
    with scope("output"):
        second_all = output(place, got3, w_output, first)
    whole2 = exchange(second_all, order)
    with scope("ff2"):
        down2, state_out, history_out = ff(
            place,
            whole2,
            second_gain.reshape(1, width),
            second_gate.T,
            second_up.T,
            second_down,
            new_state,
            new_hist,
        )
    got4 = exchange(down2, order)
    with scope("final"):
        layer_out = final(got4, second_all)
    return layer_out, state_out[None], history_out[None]


def friendly(ways, args):
    tokens, gate, taps, state, w_write = args[0], args[2], args[11], args[15], args[8]
    count, heads, head_dim, state_dim = state.shape
    return (
        count == 1
        and tokens.shape[0] == ways == 8
        and tokens.shape[1] % LANES == 0
        and gate.shape[1] % 64 == 0
        and taps.shape[1] % (8 * LANES) == 0
        and state_dim == LANES
        and LANES % head_dim == 0
        and heads < LANES
        and 2 * (w_write.shape[1] // state_dim) == 8
        and heads * head_dim % (16 * LANES) == 0
    )


def gather(block, ways):
    return exchange(jnp.broadcast_to(block[None], (ways,) + block.shape))


def scatter_sum(partial, ways):
    rows, width = partial.shape
    blocks = partial.reshape(rows, ways, width // ways).transpose(1, 0, 2)
    return jnp.sum(exchange(blocks), axis=0)


def half_block(resid, gain, w_gate, w_up, w_down, ways):
    rows = resid.shape[0]
    whole = gather(resid, ways).transpose(1, 0, 2).reshape(rows, -1)
    whole_f = whole.astype(jnp.float32)
    scale = lax.rsqrt(jnp.mean(whole_f * whole_f, axis=-1, keepdims=True) + EPS)
    normed = (whole_f * scale * gain).astype(jnp.bfloat16)
    gate = jnp.dot(normed, w_gate, preferred_element_type=jnp.float32)
    upper = jnp.dot(normed, w_up, preferred_element_type=jnp.float32)
    hidden = (jax.nn.silu(gate) * upper).astype(jnp.bfloat16)
    down = jnp.dot(hidden, w_down, preferred_element_type=jnp.float32)
    share = scatter_sum(down, ways)
    return (resid.astype(jnp.float32) + 0.5 * share).astype(jnp.bfloat16)


def make_plain(ways):
    def body(
        tokens,
        first_gain,
        first_gate,
        first_up,
        first_down,
        mix_gain,
        w_input,
        w_outgate,
        w_write,
        w_read,
        w_step,
        conv_taps,
        conv_history,
        step_bias,
        rate_log,
        mixer_state,
        group_gain,
        w_output,
        second_gain,
        second_gate,
        second_up,
        second_down,
    ):
        width = first_gate.shape[0]
        count = mixer_state.shape[0]
        heads = mixer_state.shape[1]
        head_dim = mixer_state.shape[2]
        state_dim = mixer_state.shape[3]
        ssd_width = heads * head_dim
        groups = w_write.shape[1] // state_dim
        per_group = heads // groups
        rows = tokens.shape[0]
        first = half_block(tokens, first_gain, first_gate, first_up, first_down, ways)
        first_f = first.astype(jnp.float32)
        squares = jnp.sum(first_f * first_f, axis=1, keepdims=True)
        premix = (first_f * mix_gain).astype(jnp.bfloat16)
        parts = [
            jnp.dot(premix, w, preferred_element_type=jnp.float32)
            for w in (w_input, w_write, w_read, w_outgate, w_step)
        ]
        ends = []
        total = 0
        for p in parts:
            total += p.shape[1]
            ends.append(total)
        padded = -(-(total + 1) // 1024) * 1024
        pad = jnp.zeros((rows, padded - total - 1), jnp.float32)
        packed = jnp.concatenate(parts + [squares, pad], axis=1)
        packed = packed.reshape(ways, count, padded)
        summed = jnp.sum(exchange(packed), axis=0)
        own_squares = summed[:, total : total + 1]
        scale = lax.rsqrt(own_squares / width + EPS)
        scaled = (scale * summed[:, :total]).astype(jnp.bfloat16)
        fresh = scaled[:, : ends[2]]
        outgate = scaled[:, ends[2] : ends[3]]
        steps_raw = scaled[:, ends[3] :]
        window = jnp.concatenate([conv_history, fresh[:, None, :]], axis=1)
        history_out = window[:, 1:]
        conv = jax.nn.silu(
            jnp.sum(window.astype(jnp.float32) * conv_taps.astype(jnp.float32)[None], axis=1)
        )
        conv_in = conv[:, :ssd_width].reshape(count, groups, per_group, head_dim)
        conv_write = conv[:, ssd_width : ssd_width + groups * state_dim].reshape(
            count, groups, state_dim
        )
        conv_read = conv[:, ssd_width + groups * state_dim :].reshape(count, groups, state_dim)
        step = jax.nn.softplus(steps_raw.astype(jnp.float32) + step_bias)
        decay = jnp.exp(-step * jnp.exp(rate_log))
        state = mixer_state.reshape(count, groups, per_group, head_dim, state_dim)
        decay_g = decay.reshape(count, groups, per_group)
        step_g = step.reshape(count, groups, per_group)
        written = (step_g[..., None] * conv_in)[..., None] * conv_write[:, :, None, None, :]
        new_state = decay_g[..., None, None] * state + written
        read_out = jnp.sum(new_state * conv_read[:, :, None, None, :], axis=-1)
        gated = read_out.reshape(count, ssd_width) * jax.nn.silu(outgate.astype(jnp.float32))
        blocks = gated.reshape(count, groups, ssd_width // groups)
        block_scale = lax.rsqrt(jnp.mean(blocks * blocks, axis=-1, keepdims=True) + EPS)
        normed = ((blocks * block_scale).reshape(count, ssd_width) * group_gain).astype(jnp.bfloat16)
        mixed = jnp.dot(
            gather(normed, ways).reshape(rows, ssd_width),
            w_output,
            preferred_element_type=jnp.float32,
        )
        second = (first_f + mixed).astype(jnp.bfloat16)
        layer_out = half_block(second, second_gain, second_gate, second_up, second_down, ways)
        state_out = new_state.reshape(count, heads, head_dim, state_dim)
        return (layer_out, state_out, history_out)

    return body


def solution(mesh):
    whole = P(AXES)
    rows = P(AXES, None)
    columns = P(None, AXES)
    own = ("dp",) + AXES
    kv, tp = mesh.shape["kv"], mesh.shape["tp"]
    ways = kv * tp
    leader = kv // 2 * tp + tp - 1
    plain = make_plain(ways)

    def body(*args):
        if friendly(ways, args):
            return fast_body(ways, leader, *args)
        return plain(*args)

    return jax.shard_map(
        body,
        mesh=mesh,
        in_specs=(
            P("dp", AXES),
            P(),
            columns,
            columns,
            rows,
            whole,
            rows,
            rows,
            rows,
            rows,
            rows,
            P(),
            P(own, None, None),
            P(),
            P(),
            P(own, None, None, None),
            P(),
            columns,
            P(),
            columns,
            columns,
            rows,
        ),
        out_specs=(P("dp", AXES), P(own, None, None, None), P(own, None, None)),
        check_vma=False,
    )
```

```python
import functools

import jax
import jax.numpy as jnp
from jax import lax
from jax.experimental import pallas as pl
from jax.experimental.pallas import tpu as pltpu
from jax.sharding import PartitionSpec as P

EPS = 1e-06
AXES = ("kv", "tp")
LANES = 128
MIB = 1 << 20
VMEM_SPEC = pl.BlockSpec(memory_space=pltpu.VMEM)
ROW_ROW = (((1,), (1,)), ((), ()))


def exchange(blocks, order=None):
    groups = None if order is None else [list(order)]
    return lax.all_to_all(
        blocks, AXES, split_axis=0, concat_axis=0, tiled=True, axis_index_groups=groups
    )


def params(megabytes):
    return pltpu.CompilerParams(vmem_limit_bytes=megabytes * MIB)


COST = pl.CostEstimate(flops=10**10, bytes_accessed=1000, transcendentals=0)


def silu(x):
    return x / (1.0 + jnp.exp(-x))


def repeat_kernel(block_ref, out_ref):
    for k in range(out_ref.shape[0]):
        out_ref[k] = block_ref[...]


def fetch_kernel(block_ref, out_ref):
    out_ref[...] = block_ref[...]


def fetch(block):
    return pl.pallas_call(
        fetch_kernel,
        out_shape=jax.ShapeDtypeStruct(block.shape, block.dtype),
        in_specs=[VMEM_SPEC],
        out_specs=VMEM_SPEC,
        compiler_params=params(2),
    )(block)


def repeat(block, ways):
    return pl.pallas_call(
        repeat_kernel,
        out_shape=jax.ShapeDtypeStruct((ways,) + block.shape, block.dtype),
        in_specs=[VMEM_SPEC],
        out_specs=VMEM_SPEC,
        compiler_params=params(2),
        cost_estimate=COST,
    )(block)


def ff_kernel(place, extras, x_ref, gain_ref, gate_ref, up_ref, down_ref, *refs):
    kept, out_ref, stored, sems = refs[:extras], refs[extras], refs[extras + 1 : -1], refs[-1]
    copies = [
        pltpu.make_async_copy(source, target, sems.at[i])
        for i, (source, target) in enumerate(zip(kept, stored))
    ]
    for copy in copies:
        copy.start()
    ways, rows, chan = x_ref.shape
    pieces = [x_ref[place[k]].astype(jnp.float32) for k in range(ways)]
    total = jnp.zeros((rows, 1), jnp.float32)
    for piece in pieces:
        total += jnp.sum(piece * piece, axis=1, keepdims=True)
    scale = lax.rsqrt(total / (ways * chan) + EPS)
    normed = jnp.concatenate(
        [
            (piece * gain_ref[:, k * chan : (k + 1) * chan]).astype(jnp.bfloat16)
            for k, piece in enumerate(pieces)
        ],
        axis=1,
    )
    gate = lax.dot_general(normed, gate_ref[...], ROW_ROW, preferred_element_type=jnp.float32)
    upper = lax.dot_general(normed, up_ref[...], ROW_ROW, preferred_element_type=jnp.float32)
    hidden = (silu(scale * gate) * (scale * upper)).astype(jnp.bfloat16)
    down = jnp.dot(hidden, down_ref[...], preferred_element_type=jnp.float32)
    for k in range(ways):
        out_ref[place[k]] = down[:, k * chan : (k + 1) * chan].astype(jnp.bfloat16)
    for copy in copies:
        copy.wait()


def ff(place, whole, gain, gate, up, down, *kept):
    return pl.pallas_call(
        functools.partial(ff_kernel, place, len(kept)),
        out_shape=[jax.ShapeDtypeStruct(whole.shape, jnp.bfloat16)]
        + [jax.ShapeDtypeStruct(k.shape, k.dtype) for k in kept],
        in_specs=[VMEM_SPEC] * (5 + len(kept)),
        out_specs=[VMEM_SPEC] + [pl.BlockSpec(memory_space=pltpu.HBM)] * len(kept),
        scratch_shapes=[pltpu.SemaphoreType.DMA((max(1, len(kept)),))],
        compiler_params=params(8),
        cost_estimate=COST,
    )(whole, gain, gate, up, down, *kept)


def project_kernel(place, got_ref, tok_ref, gain_ref, win_ref, wwrite_ref, wread_ref, wgate_ref, wstep_ref,
                   first_ref, out_ref, stage):
    ways, rows, chan = got_ref.shape
    slots = out_ref.shape[1]
    share = got_ref[0].astype(jnp.float32)
    for k in range(1, ways):
        share += got_ref[k].astype(jnp.float32)
    first = (tok_ref[0].astype(jnp.float32) + 0.5 * share).astype(jnp.bfloat16)
    first_ref[...] = first
    first_f = first.astype(jnp.float32)
    squares = jnp.sum(first_f * first_f, axis=1, keepdims=True)
    premix = (first_f * gain_ref[...]).astype(jnp.bfloat16)
    row = 0
    for w_ref in (win_ref, wwrite_ref, wread_ref, wgate_ref):
        part = jnp.dot(premix, w_ref[...], preferred_element_type=jnp.float32)
        for j in range(part.shape[1] // LANES):
            stage[pl.ds(row, rows, stride=slots), :] = part[:, j * LANES : (j + 1) * LANES]
            row += 1
    steps = lax.dot_general(premix, wstep_ref[...], ROW_ROW, preferred_element_type=jnp.float32)
    stage[pl.ds(row, rows, stride=slots), :] = jnp.zeros((rows, LANES), jnp.float32)
    stage[pl.ds(row, rows, stride=slots), : steps.shape[1]] = steps
    row += 1
    rest = jnp.broadcast_to(squares, (rows, LANES))
    for _ in range(3):
        term = rest.astype(jnp.bfloat16).astype(jnp.float32)
        stage[pl.ds(row, rows, stride=slots), :] = term
        rest = rest - term
        row += 1
    for j in range(row, slots):
        stage[pl.ds(j, rows, stride=slots), :] = jnp.zeros((rows, LANES), jnp.float32)
    for s in range(rows):
        out_ref[place[s]] = stage[pl.ds(s * slots, slots), :].astype(jnp.bfloat16)


def project(place, got, tokens, gain, w_in, w_write, w_read, w_gate, w_step, slots):
    ways, rows, chan = got.shape
    return pl.pallas_call(
        functools.partial(project_kernel, place),
        out_shape=[
            jax.ShapeDtypeStruct((rows, chan), jnp.bfloat16),
            jax.ShapeDtypeStruct((rows, slots, LANES), jnp.bfloat16),
        ],
        in_specs=[VMEM_SPEC] * 8,
        out_specs=[VMEM_SPEC] * 2,
        scratch_shapes=[pltpu.VMEM((rows * slots, LANES), jnp.float32)],
        compiler_params=params(8),
        cost_estimate=COST,
    )(got, tokens, gain, w_in, w_write, w_read, w_gate, w_step)


def mixer_kernel(width, groups, got_ref, taps_ref, hist_ref, bias_ref, rate_ref, state_ref, ggain_ref,
                 state_out_ref, hist_out_ref, normed_ref, read_rows, taps_rows, hist_rows, hist_wide,
                 head_rows, head_wide):
    ways = got_ref.shape[0]
    heads, head_dim, state_dim = state_ref.shape
    in_rows = heads * head_dim // LANES
    map_rows = groups * state_dim // LANES
    conv_rows = in_rows + 2 * map_rows
    taps = taps_ref.shape[0]
    for j in range(conv_rows):
        part = pl.ds(j * LANES, LANES)
        taps_rows[pl.ds(j, taps, stride=conv_rows), :] = taps_ref[:, part].astype(jnp.float32)
        hist_rows[pl.ds(j, taps - 1, stride=conv_rows), :] = hist_ref[:, part].astype(jnp.float32)
    total = got_ref[0].astype(jnp.float32)
    for k in range(1, ways):
        total += got_ref[k].astype(jnp.float32)
    step_row = conv_rows + in_rows
    squares = (
        total[step_row + 1 : step_row + 2]
        + total[step_row + 2 : step_row + 3]
        + total[step_row + 3 : step_row + 4]
    )
    scale = lax.rsqrt(squares / width + EPS)
    rounded = (total * scale).astype(jnp.bfloat16).astype(jnp.float32)
    fresh = rounded[:conv_rows]
    hist_wide[: taps - 2, :] = hist_ref[1:, :].astype(jnp.float32)
    for j in range(conv_rows):
        hist_wide[taps - 2 : taps - 1, j * LANES : (j + 1) * LANES] = fresh[j : j + 1]
    hist_out_ref[...] = hist_wide[...].astype(jnp.bfloat16)
    acc = hist_rows[pl.ds(0, conv_rows), :] * taps_rows[pl.ds(0, conv_rows), :]
    for k in range(1, taps - 1):
        part = pl.ds(k * conv_rows, conv_rows)
        acc += hist_rows[part, :] * taps_rows[part, :]
    acc += fresh * taps_rows[pl.ds((taps - 1) * conv_rows, conv_rows), :]
    conv = silu(acc)
    maps = conv[in_rows:]
    raw = rounded[step_row : step_row + 1, :heads] + bias_ref[...]
    step = jnp.maximum(raw, 0.0) + jnp.log1p(jnp.exp(-jnp.abs(raw)))
    decay = jnp.exp(-step * jnp.exp(rate_ref[...]))
    maps_high = maps.astype(jnp.bfloat16)
    maps_low = (maps - maps_high.astype(jnp.float32)).astype(jnp.bfloat16)
    maps2 = jnp.concatenate([maps_high, maps_low], axis=0)
    head_rows[...] = jnp.zeros_like(head_rows)
    head_rows[0:1, :heads] = decay
    head_rows[1:2, :heads] = step
    pad = jnp.zeros((LANES - in_rows - 8, LANES), jnp.float32)
    columns = jnp.concatenate([conv[:in_rows], head_rows[...], pad], axis=0).T
    for i in range(2):
        head_wide[i * heads : (i + 1) * heads, :] = jnp.broadcast_to(
            columns[:heads, in_rows + i : in_rows + i + 1], (heads, LANES)
        )
    per_row = LANES // head_dim
    per_group = heads // groups
    for g in range(groups):
        write = maps[g : g + 1]
        for h in range(g * per_group, (g + 1) * per_group):
            r, c = h // per_row, h % per_row
            column = columns[c * head_dim : (c + 1) * head_dim, r : r + 1]
            added = column * (head_wide[heads + h : heads + h + 1, :] * write)
            state_out_ref[h] = head_wide[h : h + 1, :] * state_ref[h] + added
        block = state_out_ref[g * per_group : (g + 1) * per_group].reshape(
            per_group * head_dim, state_dim
        )
        high = block.astype(jnp.bfloat16)
        read = lax.dot_general(maps2, high, ROW_ROW, preferred_element_type=jnp.float32)
        low = (block - high.astype(jnp.float32)).astype(jnp.bfloat16)
        read += lax.dot_general(maps2, low, ROW_ROW, preferred_element_type=jnp.float32)
        count = 2 * map_rows
        read = read[:count] + read[count:]
        span = per_group * head_dim // LANES
        for j in range(span):
            read_rows[g * span + j : g * span + j + 1, :] = read[
                map_rows + g : map_rows + g + 1, j * LANES : (j + 1) * LANES
            ]
    gated = read_rows[...] * silu(rounded[conv_rows : conv_rows + in_rows])
    sums = jnp.sum(gated * gated, axis=1, keepdims=True)
    owner = lax.broadcasted_iota(jnp.int32, (in_rows, 1), 0) // (in_rows // groups)
    block_scale = jnp.zeros((in_rows, 1), jnp.float32)
    for g in range(groups):
        mine = owner == g
        mean = jnp.sum(jnp.where(mine, sums, 0.0), axis=0, keepdims=True) / (
            in_rows // groups * LANES
        )
        block_scale = jnp.where(mine, lax.rsqrt(mean + EPS), block_scale)
    normed = (gated * block_scale * ggain_ref[...]).astype(jnp.bfloat16)
    for k in range(ways):
        normed_ref[k] = normed


def mixer(width, groups, got, taps, hist, bias, rate, state, ggain):
    ways = got.shape[0]
    heads, head_dim, state_dim = state.shape
    in_rows = heads * head_dim // LANES
    conv_rows = in_rows + 2 * groups * state_dim // LANES
    return pl.pallas_call(
        functools.partial(mixer_kernel, width, groups),
        out_shape=[
            pltpu.VMEM(state.shape, jnp.float32),
            pltpu.VMEM(hist.shape, jnp.bfloat16),
            jax.ShapeDtypeStruct((ways, in_rows, LANES), jnp.bfloat16),
        ],
        in_specs=[VMEM_SPEC] * 7,
        out_specs=[VMEM_SPEC] * 3,
        scratch_shapes=[
            pltpu.VMEM((in_rows, LANES), jnp.float32),
            pltpu.VMEM((taps.shape[0] * conv_rows, LANES), jnp.float32),
            pltpu.VMEM((hist.shape[0] * conv_rows, LANES), jnp.float32),
            pltpu.VMEM(hist.shape, jnp.float32),
            pltpu.VMEM((8, LANES), jnp.float32),
            pltpu.VMEM((2 * heads, LANES), jnp.float32),
        ],
        compiler_params=params(8),
        cost_estimate=COST,
    )(got, taps, hist, bias, rate, state, ggain)


def output_kernel(place, got_ref, w_ref, first_ref, out_ref, stage):
    ways, slots, _ = got_ref.shape
    for k in range(ways):
        stage[pl.ds(k * slots, slots), :] = got_ref[place[k]].astype(jnp.float32)
    rows = jnp.concatenate(
        [stage[pl.ds(j, ways, stride=slots), :].astype(jnp.bfloat16) for j in range(slots)], axis=1
    )
    mixed = jnp.dot(rows, w_ref[...], preferred_element_type=jnp.float32)
    second = (first_ref[...].astype(jnp.float32) + mixed).astype(jnp.bfloat16)
    for k in range(ways):
        out_ref[k] = second


def output(place, got, w, first):
    ways, slots, _ = got.shape
    return pl.pallas_call(
        functools.partial(output_kernel, place),
        out_shape=jax.ShapeDtypeStruct((ways,) + first.shape, jnp.bfloat16),
        in_specs=[VMEM_SPEC] * 3,
        out_specs=VMEM_SPEC,
        scratch_shapes=[pltpu.VMEM((ways * slots, LANES), jnp.float32)],
        compiler_params=params(4),
        cost_estimate=COST,
    )(got, w, first)


def final_kernel(got_ref, second_ref, out_ref):
    share = got_ref[0].astype(jnp.float32)
    for k in range(1, got_ref.shape[0]):
        share += got_ref[k].astype(jnp.float32)
    out_ref[...] = (second_ref[0].astype(jnp.float32) + 0.5 * share).astype(jnp.bfloat16)


def final(got, second_all):
    return pl.pallas_call(
        final_kernel,
        out_shape=jax.ShapeDtypeStruct(second_all.shape[1:], jnp.bfloat16),
        in_specs=[VMEM_SPEC] * 2,
        out_specs=VMEM_SPEC,
        compiler_params=params(2),
    )(got, second_all)


def fast_body(
    ways,
    leader,
    tokens,
    first_gain,
    first_gate,
    first_up,
    first_down,
    mix_gain,
    w_input,
    w_outgate,
    w_write,
    w_read,
    w_step,
    conv_taps,
    conv_history,
    step_bias,
    rate_log,
    mixer_state,
    group_gain,
    w_output,
    second_gain,
    second_gate,
    second_up,
    second_down,
):
    width = first_gate.shape[0]
    _, heads, head_dim, state_dim = mixer_state.shape
    groups = w_write.shape[1] // state_dim
    conv_width = conv_taps.shape[1]
    used = (conv_width + heads * head_dim) // LANES + 4
    slots = -(-used // 16) * 16
    scope = jax.named_scope
    rest = [k for k in range(ways) if k != leader]
    rest[3], rest[4] = rest[4], rest[3]
    rest[-2], rest[-1] = rest[-1], rest[-2]
    order = (leader, *rest)
    place = tuple(order.index(k) for k in range(ways))

    with scope("repeat"):
        blocks = repeat(fetch(tokens), ways)
    whole = exchange(blocks, order)
    with scope("ff1"):
        (down1,) = ff(place, whole, first_gain.reshape(1, width), first_gate.T, first_up.T, first_down)
    got1 = exchange(down1, order)
    with scope("project"):
        first, packed = project(
            place,
            got1, blocks, mix_gain.reshape(1, -1), w_input, w_write, w_read, w_outgate, w_step.T, slots
        )
    got2 = exchange(packed, order)
    with scope("mixer"):
        new_state, new_hist, normed = mixer(
            width,
            groups,
            got2,
            conv_taps,
            conv_history[0],
            step_bias.reshape(1, heads),
            rate_log.reshape(1, heads),
            mixer_state[0],
            group_gain.reshape(-1, LANES),
        )
    got3 = exchange(normed, order)
    with scope("output"):
        second_all = output(place, got3, w_output, first)
    whole2 = exchange(second_all, order)
    with scope("ff2"):
        down2, state_out, history_out = ff(
            place,
            whole2,
            second_gain.reshape(1, width),
            second_gate.T,
            second_up.T,
            second_down,
            new_state,
            new_hist,
        )
    got4 = exchange(down2, order)
    with scope("final"):
        layer_out = final(got4, second_all)
    return layer_out, state_out[None], history_out[None]


def friendly(ways, args):
    tokens, gate, taps, state, w_write = args[0], args[2], args[11], args[15], args[8]
    count, heads, head_dim, state_dim = state.shape
    return (
        count == 1
        and tokens.shape[0] == ways == 8
        and tokens.shape[1] % LANES == 0
        and gate.shape[1] % 64 == 0
        and taps.shape[1] % (8 * LANES) == 0
        and state_dim == LANES
        and LANES % head_dim == 0
        and heads < LANES
        and 2 * (w_write.shape[1] // state_dim) == 8
        and heads * head_dim % (16 * LANES) == 0
    )


def gather(block, ways):
    return exchange(jnp.broadcast_to(block[None], (ways,) + block.shape))


def scatter_sum(partial, ways):
    rows, width = partial.shape
    blocks = partial.reshape(rows, ways, width // ways).transpose(1, 0, 2)
    return jnp.sum(exchange(blocks), axis=0)


def half_block(resid, gain, w_gate, w_up, w_down, ways):
    rows = resid.shape[0]
    whole = gather(resid, ways).transpose(1, 0, 2).reshape(rows, -1)
    whole_f = whole.astype(jnp.float32)
    scale = lax.rsqrt(jnp.mean(whole_f * whole_f, axis=-1, keepdims=True) + EPS)
    normed = (whole_f * scale * gain).astype(jnp.bfloat16)
    gate = jnp.dot(normed, w_gate, preferred_element_type=jnp.float32)
    upper = jnp.dot(normed, w_up, preferred_element_type=jnp.float32)
    hidden = (jax.nn.silu(gate) * upper).astype(jnp.bfloat16)
    down = jnp.dot(hidden, w_down, preferred_element_type=jnp.float32)
    share = scatter_sum(down, ways)
    return (resid.astype(jnp.float32) + 0.5 * share).astype(jnp.bfloat16)


def make_plain(ways):
    def body(
        tokens,
        first_gain,
        first_gate,
        first_up,
        first_down,
        mix_gain,
        w_input,
        w_outgate,
        w_write,
        w_read,
        w_step,
        conv_taps,
        conv_history,
        step_bias,
        rate_log,
        mixer_state,
        group_gain,
        w_output,
        second_gain,
        second_gate,
        second_up,
        second_down,
    ):
        width = first_gate.shape[0]
        count = mixer_state.shape[0]
        heads = mixer_state.shape[1]
        head_dim = mixer_state.shape[2]
        state_dim = mixer_state.shape[3]
        ssd_width = heads * head_dim
        groups = w_write.shape[1] // state_dim
        per_group = heads // groups
        rows = tokens.shape[0]
        first = half_block(tokens, first_gain, first_gate, first_up, first_down, ways)
        first_f = first.astype(jnp.float32)
        squares = jnp.sum(first_f * first_f, axis=1, keepdims=True)
        premix = (first_f * mix_gain).astype(jnp.bfloat16)
        parts = [
            jnp.dot(premix, w, preferred_element_type=jnp.float32)
            for w in (w_input, w_write, w_read, w_outgate, w_step)
        ]
        ends = []
        total = 0
        for p in parts:
            total += p.shape[1]
            ends.append(total)
        padded = -(-(total + 1) // 1024) * 1024
        pad = jnp.zeros((rows, padded - total - 1), jnp.float32)
        packed = jnp.concatenate(parts + [squares, pad], axis=1)
        packed = packed.reshape(ways, count, padded)
        summed = jnp.sum(exchange(packed), axis=0)
        own_squares = summed[:, total : total + 1]
        scale = lax.rsqrt(own_squares / width + EPS)
        scaled = (scale * summed[:, :total]).astype(jnp.bfloat16)
        fresh = scaled[:, : ends[2]]
        outgate = scaled[:, ends[2] : ends[3]]
        steps_raw = scaled[:, ends[3] :]
        window = jnp.concatenate([conv_history, fresh[:, None, :]], axis=1)
        history_out = window[:, 1:]
        conv = jax.nn.silu(
            jnp.sum(window.astype(jnp.float32) * conv_taps.astype(jnp.float32)[None], axis=1)
        )
        conv_in = conv[:, :ssd_width].reshape(count, groups, per_group, head_dim)
        conv_write = conv[:, ssd_width : ssd_width + groups * state_dim].reshape(
            count, groups, state_dim
        )
        conv_read = conv[:, ssd_width + groups * state_dim :].reshape(count, groups, state_dim)
        step = jax.nn.softplus(steps_raw.astype(jnp.float32) + step_bias)
        decay = jnp.exp(-step * jnp.exp(rate_log))
        state = mixer_state.reshape(count, groups, per_group, head_dim, state_dim)
        decay_g = decay.reshape(count, groups, per_group)
        step_g = step.reshape(count, groups, per_group)
        written = (step_g[..., None] * conv_in)[..., None] * conv_write[:, :, None, None, :]
        new_state = decay_g[..., None, None] * state + written
        read_out = jnp.sum(new_state * conv_read[:, :, None, None, :], axis=-1)
        gated = read_out.reshape(count, ssd_width) * jax.nn.silu(outgate.astype(jnp.float32))
        blocks = gated.reshape(count, groups, ssd_width // groups)
        block_scale = lax.rsqrt(jnp.mean(blocks * blocks, axis=-1, keepdims=True) + EPS)
        normed = ((blocks * block_scale).reshape(count, ssd_width) * group_gain).astype(jnp.bfloat16)
        mixed = jnp.dot(
            gather(normed, ways).reshape(rows, ssd_width),
            w_output,
            preferred_element_type=jnp.float32,
        )
        second = (first_f + mixed).astype(jnp.bfloat16)
        layer_out = half_block(second, second_gain, second_gate, second_up, second_down, ways)
        state_out = new_state.reshape(count, heads, head_dim, state_dim)
        return (layer_out, state_out, history_out)

    return body


def solution(mesh):
    whole = P(AXES)
    rows = P(AXES, None)
    columns = P(None, AXES)
    own = ("dp",) + AXES
    kv, tp = mesh.shape["kv"], mesh.shape["tp"]
    ways = kv * tp
    leader = kv // 2 * tp + tp - 1
    plain = make_plain(ways)

    def body(*args):
        if friendly(ways, args):
            return fast_body(ways, leader, *args)
        return plain(*args)

    return jax.shard_map(
        body,
        mesh=mesh,
        in_specs=(
            P("dp", AXES),
            P(),
            columns,
            columns,
            rows,
            whole,
            rows,
            rows,
            rows,
            rows,
            rows,
            P(),
            P(own, None, None),
            P(),
            P(),
            P(own, None, None, None),
            P(),
            columns,
            P(),
            columns,
            columns,
            rows,
        ),
        out_specs=(P("dp", AXES), P(own, None, None, None), P(own, None, None)),
        check_vma=False,
    )
```

```python
import functools

import jax
import jax.numpy as jnp
from jax import lax
from jax.experimental import pallas as pl
from jax.experimental.pallas import tpu as pltpu
from jax.sharding import PartitionSpec as P

EPS = 1e-06
AXES = ("kv", "tp")
LANES = 128
MIB = 1 << 20
VMEM_SPEC = pl.BlockSpec(memory_space=pltpu.VMEM)
ROW_ROW = (((1,), (1,)), ((), ()))


def exchange(blocks, order=None):
    groups = None if order is None else [list(order)]
    return lax.all_to_all(
        blocks, AXES, split_axis=0, concat_axis=0, tiled=True, axis_index_groups=groups
    )


def params(megabytes):
    return pltpu.CompilerParams(vmem_limit_bytes=megabytes * MIB)


COST = pl.CostEstimate(flops=10**10, bytes_accessed=1000, transcendentals=0)


def silu(x):
    return x / (1.0 + jnp.exp(-x))


def repeat_kernel(block_ref, out_ref):
    for k in range(out_ref.shape[0]):
        out_ref[k] = block_ref[...]


def fetch_kernel(block_ref, out_ref):
    out_ref[...] = block_ref[...]


def fetch(block):
    return pl.pallas_call(
        fetch_kernel,
        out_shape=jax.ShapeDtypeStruct(block.shape, block.dtype),
        in_specs=[VMEM_SPEC],
        out_specs=VMEM_SPEC,
        compiler_params=params(2),
    )(block)


def repeat(block, ways):
    return pl.pallas_call(
        repeat_kernel,
        out_shape=jax.ShapeDtypeStruct((ways,) + block.shape, block.dtype),
        in_specs=[VMEM_SPEC],
        out_specs=VMEM_SPEC,
        compiler_params=params(2),
        cost_estimate=COST,
    )(block)


def ff_kernel(place, extras, x_ref, gain_ref, gate_ref, up_ref, down_ref, *refs):
    kept, out_ref, stored, sems = refs[:extras], refs[extras], refs[extras + 1 : -1], refs[-1]
    copies = [
        pltpu.make_async_copy(source, target, sems.at[i])
        for i, (source, target) in enumerate(zip(kept, stored))
    ]
    for copy in copies:
        copy.start()
    ways, rows, chan = x_ref.shape
    pieces = [x_ref[place[k]].astype(jnp.float32) for k in range(ways)]
    total = jnp.zeros((rows, 1), jnp.float32)
    for piece in pieces:
        total += jnp.sum(piece * piece, axis=1, keepdims=True)
    scale = lax.rsqrt(total / (ways * chan) + EPS)
    normed = jnp.concatenate(
        [
            (piece * gain_ref[:, k * chan : (k + 1) * chan]).astype(jnp.bfloat16)
            for k, piece in enumerate(pieces)
        ],
        axis=1,
    )
    gate = lax.dot_general(normed, gate_ref[...], ROW_ROW, preferred_element_type=jnp.float32)
    upper = lax.dot_general(normed, up_ref[...], ROW_ROW, preferred_element_type=jnp.float32)
    hidden = (silu(scale * gate) * (scale * upper)).astype(jnp.bfloat16)
    down = jnp.dot(hidden, down_ref[...], preferred_element_type=jnp.float32)
    for k in range(ways):
        out_ref[place[k]] = down[:, k * chan : (k + 1) * chan].astype(jnp.bfloat16)
    for copy in copies:
        copy.wait()


def ff(place, whole, gain, gate, up, down, *kept):
    return pl.pallas_call(
        functools.partial(ff_kernel, place, len(kept)),
        out_shape=[jax.ShapeDtypeStruct(whole.shape, jnp.bfloat16)]
        + [jax.ShapeDtypeStruct(k.shape, k.dtype) for k in kept],
        in_specs=[VMEM_SPEC] * (5 + len(kept)),
        out_specs=[VMEM_SPEC] + [pl.BlockSpec(memory_space=pltpu.HBM)] * len(kept),
        scratch_shapes=[pltpu.SemaphoreType.DMA((max(1, len(kept)),))],
        compiler_params=params(8),
        cost_estimate=COST,
    )(whole, gain, gate, up, down, *kept)


def project_kernel(place, got_ref, tok_ref, gain_ref, win_ref, wwrite_ref, wread_ref, wgate_ref, wstep_ref,
                   first_ref, out_ref, stage):
    ways, rows, chan = got_ref.shape
    slots = out_ref.shape[1]
    share = got_ref[0].astype(jnp.float32)
    for k in range(1, ways):
        share += got_ref[k].astype(jnp.float32)
    first = (tok_ref[0].astype(jnp.float32) + 0.5 * share).astype(jnp.bfloat16)
    first_ref[...] = first
    first_f = first.astype(jnp.float32)
    squares = jnp.sum(first_f * first_f, axis=1, keepdims=True)
    premix = (first_f * gain_ref[...]).astype(jnp.bfloat16)
    row = 0
    for w_ref in (win_ref, wwrite_ref, wread_ref, wgate_ref):
        part = jnp.dot(premix, w_ref[...], preferred_element_type=jnp.float32)
        for j in range(part.shape[1] // LANES):
            stage[pl.ds(row, rows, stride=slots), :] = part[:, j * LANES : (j + 1) * LANES]
            row += 1
    steps = lax.dot_general(premix, wstep_ref[...], ROW_ROW, preferred_element_type=jnp.float32)
    stage[pl.ds(row, rows, stride=slots), :] = jnp.zeros((rows, LANES), jnp.float32)
    stage[pl.ds(row, rows, stride=slots), : steps.shape[1]] = steps
    row += 1
    rest = jnp.broadcast_to(squares, (rows, LANES))
    for _ in range(3):
        term = rest.astype(jnp.bfloat16).astype(jnp.float32)
        stage[pl.ds(row, rows, stride=slots), :] = term
        rest = rest - term
        row += 1
    for j in range(row, slots):
        stage[pl.ds(j, rows, stride=slots), :] = jnp.zeros((rows, LANES), jnp.float32)
    for s in range(rows):
        out_ref[place[s]] = stage[pl.ds(s * slots, slots), :].astype(jnp.bfloat16)


def project(place, got, tokens, gain, w_in, w_write, w_read, w_gate, w_step, slots):
    ways, rows, chan = got.shape
    return pl.pallas_call(
        functools.partial(project_kernel, place),
        out_shape=[
            jax.ShapeDtypeStruct((rows, chan), jnp.bfloat16),
            jax.ShapeDtypeStruct((rows, slots, LANES), jnp.bfloat16),
        ],
        in_specs=[VMEM_SPEC] * 8,
        out_specs=[VMEM_SPEC] * 2,
        scratch_shapes=[pltpu.VMEM((rows * slots, LANES), jnp.float32)],
        compiler_params=params(8),
        cost_estimate=COST,
    )(got, tokens, gain, w_in, w_write, w_read, w_gate, w_step)


def mixer_kernel(width, groups, got_ref, taps_ref, hist_ref, bias_ref, rate_ref, state_ref, ggain_ref,
                 state_out_ref, hist_out_ref, normed_ref, read_rows, taps_rows, hist_rows, hist_wide,
                 head_rows, head_wide):
    ways = got_ref.shape[0]
    heads, head_dim, state_dim = state_ref.shape
    in_rows = heads * head_dim // LANES
    map_rows = groups * state_dim // LANES
    conv_rows = in_rows + 2 * map_rows
    taps = taps_ref.shape[0]
    for j in range(conv_rows):
        part = pl.ds(j * LANES, LANES)
        taps_rows[pl.ds(j, taps, stride=conv_rows), :] = taps_ref[:, part].astype(jnp.float32)
        hist_rows[pl.ds(j, taps - 1, stride=conv_rows), :] = hist_ref[:, part].astype(jnp.float32)
    total = got_ref[0].astype(jnp.float32)
    for k in range(1, ways):
        total += got_ref[k].astype(jnp.float32)
    step_row = conv_rows + in_rows
    squares = (
        total[step_row + 1 : step_row + 2]
        + total[step_row + 2 : step_row + 3]
        + total[step_row + 3 : step_row + 4]
    )
    scale = lax.rsqrt(squares / width + EPS)
    rounded = (total * scale).astype(jnp.bfloat16).astype(jnp.float32)
    fresh = rounded[:conv_rows]
    hist_wide[: taps - 2, :] = hist_ref[1:, :].astype(jnp.float32)
    for j in range(conv_rows):
        hist_wide[taps - 2 : taps - 1, j * LANES : (j + 1) * LANES] = fresh[j : j + 1]
    hist_out_ref[...] = hist_wide[...].astype(jnp.bfloat16)
    acc = hist_rows[pl.ds(0, conv_rows), :] * taps_rows[pl.ds(0, conv_rows), :]
    for k in range(1, taps - 1):
        part = pl.ds(k * conv_rows, conv_rows)
        acc += hist_rows[part, :] * taps_rows[part, :]
    acc += fresh * taps_rows[pl.ds((taps - 1) * conv_rows, conv_rows), :]
    conv = silu(acc)
    maps = conv[in_rows:]
    raw = rounded[step_row : step_row + 1, :heads] + bias_ref[...]
    step = jnp.maximum(raw, 0.0) + jnp.log1p(jnp.exp(-jnp.abs(raw)))
    decay = jnp.exp(-step * jnp.exp(rate_ref[...]))
    maps_high = maps.astype(jnp.bfloat16)
    maps_low = (maps - maps_high.astype(jnp.float32)).astype(jnp.bfloat16)
    maps2 = jnp.concatenate([maps_high, maps_low], axis=0)
    head_rows[...] = jnp.zeros_like(head_rows)
    head_rows[0:1, :heads] = decay
    head_rows[1:2, :heads] = step
    pad = jnp.zeros((LANES - in_rows - 8, LANES), jnp.float32)
    columns = jnp.concatenate([conv[:in_rows], head_rows[...], pad], axis=0).T
    for i in range(2):
        head_wide[i * heads : (i + 1) * heads, :] = jnp.broadcast_to(
            columns[:heads, in_rows + i : in_rows + i + 1], (heads, LANES)
        )
    per_row = LANES // head_dim
    per_group = heads // groups
    for g in range(groups):
        write = maps[g : g + 1]
        for h in range(g * per_group, (g + 1) * per_group):
            r, c = h // per_row, h % per_row
            column = columns[c * head_dim : (c + 1) * head_dim, r : r + 1]
            added = column * (head_wide[heads + h : heads + h + 1, :] * write)
            state_out_ref[h] = head_wide[h : h + 1, :] * state_ref[h] + added
        block = state_out_ref[g * per_group : (g + 1) * per_group].reshape(
            per_group * head_dim, state_dim
        )
        high = block.astype(jnp.bfloat16)
        read = lax.dot_general(maps2, high, ROW_ROW, preferred_element_type=jnp.float32)
        count = 2 * map_rows
        read = read[:count] + read[count:]
        span = per_group * head_dim // LANES
        for j in range(span):
            read_rows[g * span + j : g * span + j + 1, :] = read[
                map_rows + g : map_rows + g + 1, j * LANES : (j + 1) * LANES
            ]
    gated = read_rows[...] * silu(rounded[conv_rows : conv_rows + in_rows])
    sums = jnp.sum(gated * gated, axis=1, keepdims=True)
    owner = lax.broadcasted_iota(jnp.int32, (in_rows, 1), 0) // (in_rows // groups)
    block_scale = jnp.zeros((in_rows, 1), jnp.float32)
    for g in range(groups):
        mine = owner == g
        mean = jnp.sum(jnp.where(mine, sums, 0.0), axis=0, keepdims=True) / (
            in_rows // groups * LANES
        )
        block_scale = jnp.where(mine, lax.rsqrt(mean + EPS), block_scale)
    normed = (gated * block_scale * ggain_ref[...]).astype(jnp.bfloat16)
    for k in range(ways):
        normed_ref[k] = normed


def mixer(width, groups, got, taps, hist, bias, rate, state, ggain):
    ways = got.shape[0]
    heads, head_dim, state_dim = state.shape
    in_rows = heads * head_dim // LANES
    conv_rows = in_rows + 2 * groups * state_dim // LANES
    return pl.pallas_call(
        functools.partial(mixer_kernel, width, groups),
        out_shape=[
            pltpu.VMEM(state.shape, jnp.float32),
            pltpu.VMEM(hist.shape, jnp.bfloat16),
            jax.ShapeDtypeStruct((ways, in_rows, LANES), jnp.bfloat16),
        ],
        in_specs=[VMEM_SPEC] * 7,
        out_specs=[VMEM_SPEC] * 3,
        scratch_shapes=[
            pltpu.VMEM((in_rows, LANES), jnp.float32),
            pltpu.VMEM((taps.shape[0] * conv_rows, LANES), jnp.float32),
            pltpu.VMEM((hist.shape[0] * conv_rows, LANES), jnp.float32),
            pltpu.VMEM(hist.shape, jnp.float32),
            pltpu.VMEM((8, LANES), jnp.float32),
            pltpu.VMEM((2 * heads, LANES), jnp.float32),
        ],
        compiler_params=params(8),
        cost_estimate=COST,
    )(got, taps, hist, bias, rate, state, ggain)


def output_kernel(place, got_ref, w_ref, first_ref, out_ref, stage):
    ways, slots, _ = got_ref.shape
    for k in range(ways):
        stage[pl.ds(k * slots, slots), :] = got_ref[place[k]].astype(jnp.float32)
    rows = jnp.concatenate(
        [stage[pl.ds(j, ways, stride=slots), :].astype(jnp.bfloat16) for j in range(slots)], axis=1
    )
    mixed = jnp.dot(rows, w_ref[...], preferred_element_type=jnp.float32)
    second = (first_ref[...].astype(jnp.float32) + mixed).astype(jnp.bfloat16)
    for k in range(ways):
        out_ref[k] = second


def output(place, got, w, first):
    ways, slots, _ = got.shape
    return pl.pallas_call(
        functools.partial(output_kernel, place),
        out_shape=jax.ShapeDtypeStruct((ways,) + first.shape, jnp.bfloat16),
        in_specs=[VMEM_SPEC] * 3,
        out_specs=VMEM_SPEC,
        scratch_shapes=[pltpu.VMEM((ways * slots, LANES), jnp.float32)],
        compiler_params=params(4),
        cost_estimate=COST,
    )(got, w, first)


def final_kernel(got_ref, second_ref, out_ref):
    share = got_ref[0].astype(jnp.float32)
    for k in range(1, got_ref.shape[0]):
        share += got_ref[k].astype(jnp.float32)
    out_ref[...] = (second_ref[0].astype(jnp.float32) + 0.5 * share).astype(jnp.bfloat16)


def final(got, second_all):
    return pl.pallas_call(
        final_kernel,
        out_shape=jax.ShapeDtypeStruct(second_all.shape[1:], jnp.bfloat16),
        in_specs=[VMEM_SPEC] * 2,
        out_specs=VMEM_SPEC,
        compiler_params=params(2),
    )(got, second_all)


def fast_body(
    ways,
    leader,
    tokens,
    first_gain,
    first_gate,
    first_up,
    first_down,
    mix_gain,
    w_input,
    w_outgate,
    w_write,
    w_read,
    w_step,
    conv_taps,
    conv_history,
    step_bias,
    rate_log,
    mixer_state,
    group_gain,
    w_output,
    second_gain,
    second_gate,
    second_up,
    second_down,
):
    width = first_gate.shape[0]
    _, heads, head_dim, state_dim = mixer_state.shape
    groups = w_write.shape[1] // state_dim
    conv_width = conv_taps.shape[1]
    used = (conv_width + heads * head_dim) // LANES + 4
    slots = -(-used // 16) * 16
    scope = jax.named_scope
    rest = [k for k in range(ways) if k != leader]
    rest[3], rest[4] = rest[4], rest[3]
    rest[-2], rest[-1] = rest[-1], rest[-2]
    order = (leader, *rest)
    place = tuple(order.index(k) for k in range(ways))

    with scope("repeat"):
        blocks = repeat(fetch(tokens), ways)
    whole = exchange(blocks, order)
    with scope("ff1"):
        (down1,) = ff(place, whole, first_gain.reshape(1, width), first_gate.T, first_up.T, first_down)
    got1 = exchange(down1, order)
    with scope("project"):
        first, packed = project(
            place,
            got1, blocks, mix_gain.reshape(1, -1), w_input, w_write, w_read, w_outgate, w_step.T, slots
        )
    got2 = exchange(packed, order)
    with scope("mixer"):
        new_state, new_hist, normed = mixer(
            width,
            groups,
            got2,
            conv_taps,
            conv_history[0],
            step_bias.reshape(1, heads),
            rate_log.reshape(1, heads),
            mixer_state[0],
            group_gain.reshape(-1, LANES),
        )
    got3 = exchange(normed, order)
    with scope("output"):
        second_all = output(place, got3, w_output, first)
    whole2 = exchange(second_all, order)
    with scope("ff2"):
        down2, state_out, history_out = ff(
            place,
            whole2,
            second_gain.reshape(1, width),
            second_gate.T,
            second_up.T,
            second_down,
            new_state,
            new_hist,
        )
    got4 = exchange(down2, order)
    with scope("final"):
        layer_out = final(got4, second_all)
    return layer_out, state_out[None], history_out[None]


def friendly(ways, args):
    tokens, gate, taps, state, w_write = args[0], args[2], args[11], args[15], args[8]
    count, heads, head_dim, state_dim = state.shape
    return (
        count == 1
        and tokens.shape[0] == ways == 8
        and tokens.shape[1] % LANES == 0
        and gate.shape[1] % 64 == 0
        and taps.shape[1] % (8 * LANES) == 0
        and state_dim == LANES
        and LANES % head_dim == 0
        and heads < LANES
        and 2 * (w_write.shape[1] // state_dim) == 8
        and heads * head_dim % (16 * LANES) == 0
    )


def gather(block, ways):
    return exchange(jnp.broadcast_to(block[None], (ways,) + block.shape))


def scatter_sum(partial, ways):
    rows, width = partial.shape
    blocks = partial.reshape(rows, ways, width // ways).transpose(1, 0, 2)
    return jnp.sum(exchange(blocks), axis=0)


def half_block(resid, gain, w_gate, w_up, w_down, ways):
    rows = resid.shape[0]
    whole = gather(resid, ways).transpose(1, 0, 2).reshape(rows, -1)
    whole_f = whole.astype(jnp.float32)
    scale = lax.rsqrt(jnp.mean(whole_f * whole_f, axis=-1, keepdims=True) + EPS)
    normed = (whole_f * scale * gain).astype(jnp.bfloat16)
    gate = jnp.dot(normed, w_gate, preferred_element_type=jnp.float32)
    upper = jnp.dot(normed, w_up, preferred_element_type=jnp.float32)
    hidden = (jax.nn.silu(gate) * upper).astype(jnp.bfloat16)
    down = jnp.dot(hidden, w_down, preferred_element_type=jnp.float32)
    share = scatter_sum(down, ways)
    return (resid.astype(jnp.float32) + 0.5 * share).astype(jnp.bfloat16)


def make_plain(ways):
    def body(
        tokens,
        first_gain,
        first_gate,
        first_up,
        first_down,
        mix_gain,
        w_input,
        w_outgate,
        w_write,
        w_read,
        w_step,
        conv_taps,
        conv_history,
        step_bias,
        rate_log,
        mixer_state,
        group_gain,
        w_output,
        second_gain,
        second_gate,
        second_up,
        second_down,
    ):
        width = first_gate.shape[0]
        count = mixer_state.shape[0]
        heads = mixer_state.shape[1]
        head_dim = mixer_state.shape[2]
        state_dim = mixer_state.shape[3]
        ssd_width = heads * head_dim
        groups = w_write.shape[1] // state_dim
        per_group = heads // groups
        rows = tokens.shape[0]
        first = half_block(tokens, first_gain, first_gate, first_up, first_down, ways)
        first_f = first.astype(jnp.float32)
        squares = jnp.sum(first_f * first_f, axis=1, keepdims=True)
        premix = (first_f * mix_gain).astype(jnp.bfloat16)
        parts = [
            jnp.dot(premix, w, preferred_element_type=jnp.float32)
            for w in (w_input, w_write, w_read, w_outgate, w_step)
        ]
        ends = []
        total = 0
        for p in parts:
            total += p.shape[1]
            ends.append(total)
        padded = -(-(total + 1) // 1024) * 1024
        pad = jnp.zeros((rows, padded - total - 1), jnp.float32)
        packed = jnp.concatenate(parts + [squares, pad], axis=1)
        packed = packed.reshape(ways, count, padded)
        summed = jnp.sum(exchange(packed), axis=0)
        own_squares = summed[:, total : total + 1]
        scale = lax.rsqrt(own_squares / width + EPS)
        scaled = (scale * summed[:, :total]).astype(jnp.bfloat16)
        fresh = scaled[:, : ends[2]]
        outgate = scaled[:, ends[2] : ends[3]]
        steps_raw = scaled[:, ends[3] :]
        window = jnp.concatenate([conv_history, fresh[:, None, :]], axis=1)
        history_out = window[:, 1:]
        conv = jax.nn.silu(
            jnp.sum(window.astype(jnp.float32) * conv_taps.astype(jnp.float32)[None], axis=1)
        )
        conv_in = conv[:, :ssd_width].reshape(count, groups, per_group, head_dim)
        conv_write = conv[:, ssd_width : ssd_width + groups * state_dim].reshape(
            count, groups, state_dim
        )
        conv_read = conv[:, ssd_width + groups * state_dim :].reshape(count, groups, state_dim)
        step = jax.nn.softplus(steps_raw.astype(jnp.float32) + step_bias)
        decay = jnp.exp(-step * jnp.exp(rate_log))
        state = mixer_state.reshape(count, groups, per_group, head_dim, state_dim)
        decay_g = decay.reshape(count, groups, per_group)
        step_g = step.reshape(count, groups, per_group)
        written = (step_g[..., None] * conv_in)[..., None] * conv_write[:, :, None, None, :]
        new_state = decay_g[..., None, None] * state + written
        read_out = jnp.sum(new_state * conv_read[:, :, None, None, :], axis=-1)
        gated = read_out.reshape(count, ssd_width) * jax.nn.silu(outgate.astype(jnp.float32))
        blocks = gated.reshape(count, groups, ssd_width // groups)
        block_scale = lax.rsqrt(jnp.mean(blocks * blocks, axis=-1, keepdims=True) + EPS)
        normed = ((blocks * block_scale).reshape(count, ssd_width) * group_gain).astype(jnp.bfloat16)
        mixed = jnp.dot(
            gather(normed, ways).reshape(rows, ssd_width),
            w_output,
            preferred_element_type=jnp.float32,
        )
        second = (first_f + mixed).astype(jnp.bfloat16)
        layer_out = half_block(second, second_gain, second_gate, second_up, second_down, ways)
        state_out = new_state.reshape(count, heads, head_dim, state_dim)
        return (layer_out, state_out, history_out)

    return body


def solution(mesh):
    whole = P(AXES)
    rows = P(AXES, None)
    columns = P(None, AXES)
    own = ("dp",) + AXES
    kv, tp = mesh.shape["kv"], mesh.shape["tp"]
    ways = kv * tp
    leader = kv // 2 * tp + tp - 1
    plain = make_plain(ways)

    def body(*args):
        if friendly(ways, args):
            return fast_body(ways, leader, *args)
        return plain(*args)

    return jax.shard_map(
        body,
        mesh=mesh,
        in_specs=(
            P("dp", AXES),
            P(),
            columns,
            columns,
            rows,
            whole,
            rows,
            rows,
            rows,
            rows,
            rows,
            P(),
            P(own, None, None),
            P(),
            P(),
            P(own, None, None, None),
            P(),
            columns,
            P(),
            columns,
            columns,
            rows,
        ),
        out_specs=(P("dp", AXES), P(own, None, None, None), P(own, None, None)),
        check_vma=False,
    )
```
